128 devices in a mesh: sp: 64 (over z, y, x), tp: 2 (over core).
Axes of the slice: x: 4, y: 4, z: 4, core: 2. Of those that a mesh axis runs over, the one named last changes fastest.
Arguments:
- query_matrix: bfloat16 [16384, 2048], P('sp', 'tp'), may hold values from -6 to 6
- key_matrix: bfloat16 [16384, 2048], P('sp', 'tp'), may hold values from -6 to 6
- value_matrix: bfloat16 [16384, 2048], P('sp', 'tp'), may hold values from -6 to 6
- output_gate_logits: bfloat16 [16384, 2048], P('sp', 'tp'), may hold values from -6 to 6
- decay_preactivation: bfloat16 [16384, 2048], P('sp', 'tp'), may hold values from -3 to 12
- head_extra_decay: float32 [16384, 32], P('sp', 'tp'), may hold values from -0.7 to 0
- residual: bfloat16 [16384, 2048], P(('sp', 'tp')), may hold values from -6 to 6
- head_norm_gain: float32 [64], replicated, may hold values from 0.1 to 1.9
- output_projection_weight: bfloat16 [2048, 2048], P('tp'), may hold values from -0.125 to 0.125
- mixer_norm_gain: float32 [2048], replicated, may hold values from 0.1 to 1.9
- routes: int32 [16384, 2], P(('sp', 'tp')), may hold values from 0 to 63, all different within a row; in each aligned block of 128 rows (0 to 127, 128 to 255, ...) at most 8 rows name the same one
- routing_weight: float32 [16384, 2], P(('sp', 'tp')), may hold values from 0.2 to 1.5
- routed_gate_weight: bfloat16 [64, 2048, 1024], P('sp', None, 'tp'), may hold values from -0.125 to 0.125
- routed_up_weight: bfloat16 [64, 2048, 1024], P('sp', None, 'tp'), may hold values from -0.125 to 0.125
- routed_down_weight: bfloat16 [64, 1024, 2048], P('sp', 'tp'), may hold values from -0.1875 to 0.1875
- common_gate_weight: bfloat16 [2048, 512], replicated, may hold values from -0.125 to 0.125
- common_up_weight: bfloat16 [2048, 512], replicated, may hold values from -0.125 to 0.125
- common_down_weight: bfloat16 [512, 2048], replicated, may hold values from -0.25 to 0.25
- final_norm_gain: float32 [2048], replicated, may hold values from 0.1 to 1.9
Outputs:
- layer_out: bfloat16 [16384, 2048], P(('sp', 'tp'))
The draws below stay inside these ranges and needn't reach their ends.
Inputs may be any that keep to these rules, and one draw needn't show every extreme that they name: `routes`: each row names 2 different experts. In the rows of one device (aligned blocks of rows) no expert is named by more than 8 rows, a bound that some block reaches.
All inputs are finite; a program needn't handle non-finite values.
Results may differ from the reference program's by a relative error of at most 0.019.
Values may be sent and summed in bfloat16 or wider, within the bound.
A program may use at most 192 MiB of HBM per device.

```python
import math
import jax
import jax.numpy as jnp
import numpy as np
from jax import lax

D = 2048
HEAD_NUMBER = 32
KEY_HEAD_SIZE = 64
BLOCK_TOKENS = 64
FE = 1024
FS = 512
TOP_K = 2
TOK_DEV = 256
SEQUENCE_TOKENS = 16384
EXPERTS = 64
CAP = 8
N_SP = 64
N_TP = 2


def draw_decay_preactivation(key, part):
    head_key, fast_key, slow_key, device_key, noise_key = jax.random.split(key, 5)
    fast_share = 0.5
    fast_head = jax.random.uniform(head_key, (HEAD_NUMBER,), jnp.float32) < fast_share
    fast_level = jax.random.uniform(fast_key, (HEAD_NUMBER, KEY_HEAD_SIZE), jnp.float32, -0.5, 1.0)
    slow_level = math.log(SEQUENCE_TOKENS / 9.6) + jax.random.uniform(slow_key, (HEAD_NUMBER, KEY_HEAD_SIZE), jnp.float32, -0.7, 0.7)
    level = jnp.where(fast_head[:, None], fast_level, slow_level).reshape(1, HEAD_NUMBER * KEY_HEAD_SIZE)
    device_shift = jax.random.uniform(device_key, (SEQUENCE_TOKENS // TOK_DEV, 1), jnp.float32, -0.7, 0.7)
    device_shift = jnp.repeat(device_shift, TOK_DEV, axis=0, total_repeat_length=SEQUENCE_TOKENS)
    noise = 0.7 * jax.random.normal(noise_key, (SEQUENCE_TOKENS, HEAD_NUMBER * KEY_HEAD_SIZE), jnp.float32)
    return jnp.clip(level + device_shift + noise, -3.0, 12.0).astype(jnp.bfloat16)


def draw_head_extra_decay(key, part):
    place_key, dropout_random_key = jax.random.split(key)
    places = jax.random.randint(place_key, (8,), 0, SEQUENCE_TOKENS)
    removed_entries = jnp.any(jnp.arange(SEQUENCE_TOKENS)[:, None] == places[None, :], axis=1)
    spike_dropped = jax.random.uniform(dropout_random_key, (SEQUENCE_TOKENS, HEAD_NUMBER), jnp.float32, -0.7, -0.22)
    return jnp.where(removed_entries[:, None], spike_dropped, 0.0).astype(jnp.float32)


def steps_of(key, dims, pieces, least, top_value):
    factor_of = 1.0
    for position, shards_of in pieces:
        heights = jax.random.uniform(jax.random.fold_in(jax.random.fold_in(key, 6), position), (shards_of,), jnp.float32, least / len(pieces), top_value / len(pieces))
        factor_of = factor_of * jnp.repeat(jnp.exp(heights), dims[position] // shards_of).reshape((-1,) + (1,) * (len(dims) - 1 - position))
    return factor_of


def shared_out(key, own, number, rows, amount, top, most, lean):
    sequence = jax.random.permutation(key, amount)
    heavy_load, common = shares(amount, rows * top, most, lean, True), shares(amount, rows * top, most, lean, False)
    places = jnp.arange(amount)

    def named(lengths, turn):
        used = int((lengths > 0).sum())
        fixed = max(1, used // 4)
        shifted = fixed + (places - fixed + turn * (used - fixed)) % max(1, amount - fixed)
        return jnp.zeros((amount,), jnp.int32).at[sequence[jnp.where(places < fixed, places, shifted)]].set(jnp.asarray(lengths, jnp.int32))

    lengths = jnp.where(number % 4 == 0, named(heavy_load, number // 4), named(common, number - number // 4 - 1))
    mixed = jax.random.permutation(jax.random.fold_in(own, 3), amount)
    donor, receiver = mixed[0:amount // 2 * 2:2], mixed[1:amount // 2 * 2:2]
    room = jnp.minimum(lengths[donor] - 1, most - lengths[receiver]) // 2
    room = jnp.where((donor == sequence[0]) | (receiver == sequence[0]) | (lengths[receiver] == 0), 0, jnp.maximum(room, 0))
    shifted = jax.random.randint(jax.random.fold_in(own, 4), (amount // 2,), 0, 1 << 20) % (room + 1)
    lengths = lengths.at[donor].add(-shifted).at[receiver].add(shifted)
    labels = jnp.searchsorted(jnp.cumsum(lengths), jnp.arange(rows * top), side="right").astype(jnp.int32)
    grid = labels.reshape(top, rows).T
    grid = grid[jax.random.permutation(jax.random.fold_in(own, 1), rows)]
    turn = jax.random.randint(jax.random.fold_in(own, 2), (rows, 1), 0, top)
    return jnp.take_along_axis(grid, (jnp.arange(top)[None, :] + turn) % top, axis=1)


def shares(amount, total, bound, lean, full):
    portions = [(1 << 20) // math.isqrt(rank ** lean) + 1 for rank in range(1, amount + 1)]
    largest = bound if full else min(bound, max(-(-total // amount), total * portions[0] // sum(portions)))
    least = 1 if total - largest >= amount - 1 else 0
    given, spare = [largest] + [least] * (amount - 1), total - largest - least * (amount - 1)
    while spare > 0:
        free = [i for i in range(1, amount) if given[i] < largest] or [i for i in range(1, amount) if given[i] < bound]
        whole, budget = sum([portions[i] for i in free]), spare
        for i in free:
            addition = min(bound - given[i], max(1, budget * portions[i] // whole), spare)
            given[i] = given[i] + addition
            spare = spare - addition
    return np.array(given)


def bell_draw(stream_key, dims, width, bound, cuts=(), kind=jnp.bfloat16):
    entries = width * jax.random.normal(stream_key, dims, jnp.float32)
    if cuts:
        entries = entries * steps_of(stream_key, dims, cuts, -0.22, 0.18)
    return jnp.clip(entries, -bound, bound).astype(kind)


def setup_inputs(seed: int = 0) -> dict:
    streams_of = jax.random.split(jax.random.key(seed), 20)
    query_matrix = bell_draw(streams_of[0], (SEQUENCE_TOKENS, HEAD_NUMBER * KEY_HEAD_SIZE), 1.0, 6.0, ((0, 64), (1, 2)))
    key_matrix = bell_draw(streams_of[1], (SEQUENCE_TOKENS, HEAD_NUMBER * KEY_HEAD_SIZE), 1.0, 6.0, ((0, 64), (1, 2)))
    value_matrix = bell_draw(streams_of[2], (SEQUENCE_TOKENS, HEAD_NUMBER * KEY_HEAD_SIZE), 1.0, 6.0, ((0, 64), (1, 2)))
    output_gate_logits = bell_draw(streams_of[3], (SEQUENCE_TOKENS, HEAD_NUMBER * KEY_HEAD_SIZE), 1.0, 6.0, ((0, 64), (1, 2)))
    decay_preactivation = draw_decay_preactivation(jax.random.fold_in(streams_of[19], 71), 0)
    head_extra_decay = draw_head_extra_decay(jax.random.fold_in(streams_of[19], 71), 0)
    residual = bell_draw(streams_of[6], (SEQUENCE_TOKENS, D), 1.0, 6.0, ((0, 128),))
    head_norm_gain = jnp.clip(1.0 + 0.18 * jax.random.normal(streams_of[7], (KEY_HEAD_SIZE,), jnp.float32), 0.1, 1.9)
    output_projection_weight = bell_draw(streams_of[8], (HEAD_NUMBER * KEY_HEAD_SIZE, D), (HEAD_NUMBER * KEY_HEAD_SIZE) ** -0.5, 0.125, ((0, 2),))
    mixer_norm_gain = jnp.clip(1.0 + 0.18 * jax.random.normal(streams_of[9], (D,), jnp.float32), 0.1, 1.9)
    routes_keys = jax.random.split(jax.random.fold_in(streams_of[10], 1), SEQUENCE_TOKENS // (TOK_DEV // N_TP))
    routes_turns = jax.random.permutation(jax.random.fold_in(streams_of[10], 3), SEQUENCE_TOKENS // (TOK_DEV // N_TP))
    routes = jax.vmap(lambda own, number: shared_out(jax.random.fold_in(streams_of[10], 2), own, number, TOK_DEV // N_TP, EXPERTS, TOP_K, CAP, 1))(routes_keys, routes_turns).reshape((SEQUENCE_TOKENS, TOP_K))
    routing_weight = jnp.clip(0.2 + 1.3 * jax.random.uniform(streams_of[11], (SEQUENCE_TOKENS, TOP_K), jnp.float32) ** steps_of(streams_of[11], (SEQUENCE_TOKENS, TOP_K), ((0, 128),), -0.2, 0.2), 0.2, 1.5)
    routed_gate_weight = bell_draw(streams_of[12], (EXPERTS, D, FE), D ** -0.5, 0.125, ((0, 64), (2, 2)))
    routed_up_weight = bell_draw(streams_of[13], (EXPERTS, D, FE), D ** -0.5, 0.125, ((0, 64), (2, 2)))
    routed_down_weight = bell_draw(streams_of[14], (EXPERTS, FE, D), FE ** -0.5, 0.1875, ((0, 64), (1, 2)))
    common_gate_weight = bell_draw(streams_of[15], (D, FS), D ** -0.5, 0.125)
    common_up_weight = bell_draw(streams_of[16], (D, FS), D ** -0.5, 0.125)
    common_down_weight = bell_draw(streams_of[17], (FS, D), FS ** -0.5, 0.25)
    final_norm_gain = jnp.clip(1.0 + 0.18 * jax.random.normal(streams_of[18], (D,), jnp.float32), 0.1, 1.9)
    return {"query_matrix": query_matrix, "key_matrix": key_matrix, "value_matrix": value_matrix, "output_gate_logits": output_gate_logits, "decay_preactivation": decay_preactivation, "head_extra_decay": head_extra_decay, "residual": residual, "head_norm_gain": head_norm_gain, "output_projection_weight": output_projection_weight, "mixer_norm_gain": mixer_norm_gain, "routes": routes, "routing_weight": routing_weight, "routed_gate_weight": routed_gate_weight, "routed_up_weight": routed_up_weight, "routed_down_weight": routed_down_weight, "common_gate_weight": common_gate_weight, "common_up_weight": common_up_weight, "common_down_weight": common_down_weight, "final_norm_gain": final_norm_gain}


EPS = 1e-06
GATE_DIVISOR = 16.0

def round_half(values):
    return lax.optimization_barrier(values.astype(jnp.bfloat16)).astype(jnp.float32)

def layer_norm(values, gain):
    center = values - lax.optimization_barrier(jnp.mean(values, axis=-1, keepdims=True))
    spread = lax.optimization_barrier(jnp.mean(center * center, axis=-1, keepdims=True))
    return center * lax.rsqrt(spread + EPS) * gain

def prepare_inputs(blocked_queries, blocked_keys, blocked_decay, spike_block_decay):
    logarithm_decay = jax.nn.log_sigmoid(blocked_decay.astype(jnp.float32)).reshape(BLOCK_TOKENS, HEAD_NUMBER, KEY_HEAD_SIZE) / GATE_DIVISOR
    logarithm_decay = logarithm_decay + spike_block_decay[:, :, None]
    inside_block = jnp.cumsum(logarithm_decay, axis=0)
    query_float = blocked_queries.astype(jnp.float32).reshape(BLOCK_TOKENS, HEAD_NUMBER, KEY_HEAD_SIZE) * KEY_HEAD_SIZE ** (-0.5)
    key_float = blocked_keys.astype(jnp.float32).reshape(BLOCK_TOKENS, HEAD_NUMBER, KEY_HEAD_SIZE)
    return (inside_block, query_float, key_float)

def forward_block(left_state, fragments):
    blocked_queries, blocked_keys, blocked_values, blocked_decay, spike_block_decay = fragments
    inside_block, query_float, key_float = prepare_inputs(blocked_queries, blocked_keys, blocked_decay, spike_block_decay)
    value_f = blocked_values.astype(jnp.float32).reshape(BLOCK_TOKENS, HEAD_NUMBER, KEY_HEAD_SIZE)
    total = inside_block[-1]
    query_up = query_float * jnp.exp(inside_block)
    query_down = query_float * jnp.exp(-inside_block)
    key_up = key_float * jnp.exp(inside_block)
    key_down = key_float * jnp.exp(-inside_block)
    lower_mask = jnp.tril(jnp.ones((BLOCK_TOKENS, BLOCK_TOKENS), bool))
    ahead = jnp.einsum('ihc,jhc->hij', query_up, key_down)
    behind = jnp.einsum('ihc,jhc->hij', query_down, key_up)
    scores = jnp.where(lower_mask, ahead, 0.0) + jnp.where(lower_mask, 0.0, behind)
    block_out = jnp.einsum('hij,jhv->ihv', scores, value_f)
    block_out = block_out + jnp.einsum('ihc,hcv->ihv', query_up, left_state)
    key_end = key_float * jnp.exp(total[None] - inside_block)
    new_state = jnp.exp(total)[..., None] * left_state + jnp.einsum('jhc,jhv->hcv', key_end, value_f)
    return (new_state, block_out)

def backward_block(right_state, fragments):
    blocked_queries, blocked_keys, blocked_values, blocked_decay, spike_block_decay = fragments
    inside_block, query_float, key_float = prepare_inputs(blocked_queries, blocked_keys, blocked_decay, spike_block_decay)
    value_f = blocked_values.astype(jnp.float32).reshape(BLOCK_TOKENS, HEAD_NUMBER, KEY_HEAD_SIZE)
    total = inside_block[-1]
    query_tail = query_float * jnp.exp(total[None] - inside_block)
    block_out = jnp.einsum('ihc,hcv->ihv', query_tail, right_state)
    key_up = key_float * jnp.exp(inside_block)
    new_state = jnp.exp(total)[..., None] * right_state + jnp.einsum('jhc,jhv->hcv', key_up, value_f)
    return (new_state, block_out)

def reference(query_matrix, key_matrix, value_matrix, output_gate_logits, decay_preactivation, head_extra_decay, residual, head_norm_gain, output_projection_weight, mixer_norm_gain, routes, routing_weight, routed_gate_weight, routed_up_weight, routed_down_weight, common_gate_weight, common_up_weight, common_down_weight, final_norm_gain):
    token_count = query_matrix.shape[0]
    number_of_blocks = token_count // BLOCK_TOKENS
    fragments = (query_matrix.reshape(number_of_blocks, BLOCK_TOKENS, HEAD_NUMBER * KEY_HEAD_SIZE), key_matrix.reshape(number_of_blocks, BLOCK_TOKENS, HEAD_NUMBER * KEY_HEAD_SIZE), value_matrix.reshape(number_of_blocks, BLOCK_TOKENS, HEAD_NUMBER * KEY_HEAD_SIZE), decay_preactivation.reshape(number_of_blocks, BLOCK_TOKENS, HEAD_NUMBER * KEY_HEAD_SIZE), head_extra_decay.reshape(number_of_blocks, BLOCK_TOKENS, HEAD_NUMBER))
    zero_state = jnp.zeros((HEAD_NUMBER, KEY_HEAD_SIZE, KEY_HEAD_SIZE), jnp.float32)
    _, forward_out = lax.scan(forward_block, zero_state, fragments)
    _, backward_out = lax.scan(backward_block, zero_state, fragments, reverse=True)
    mixed = (forward_out + backward_out).reshape(token_count, HEAD_NUMBER, KEY_HEAD_SIZE)
    normed_heads = mixed * lax.rsqrt(lax.optimization_barrier(jnp.mean(mixed * mixed, axis=-1, keepdims=True)) + EPS) * head_norm_gain
    gated = (normed_heads.reshape(token_count, HEAD_NUMBER * KEY_HEAD_SIZE) * jax.nn.silu(output_gate_logits.astype(jnp.float32))).astype(jnp.bfloat16)
    group_width = HEAD_NUMBER * KEY_HEAD_SIZE // N_TP
    projected = jnp.zeros((token_count, D), jnp.float32)
    for group in range(N_TP):
        part_sum = jnp.dot(gated[:, group * group_width:(group + 1) * group_width], output_projection_weight[group * group_width:(group + 1) * group_width], preferred_element_type=jnp.float32)
        projected = projected + round_half(part_sum)
    normed = layer_norm(residual.astype(jnp.float32) + projected, mixer_norm_gain).astype(jnp.bfloat16)
    sources = N_SP * N_TP
    row_count = TOK_DEV // N_TP
    assigned = row_count * TOP_K
    flat_routes = routes.reshape(sources, assigned)
    member = (flat_routes[:, :, None] == jnp.arange(EXPERTS, dtype=jnp.int32)[None, None, :]).astype(jnp.int32)
    rank_in = lax.optimization_barrier(jnp.sum((jnp.cumsum(member, axis=1) - member) * member, axis=2))
    column = jnp.arange(sources, dtype=jnp.int32)[:, None] * CAP + rank_in
    token_index = jnp.arange(sources, dtype=jnp.int32)[:, None] * row_count + jnp.arange(assigned, dtype=jnp.int32)[None, :] // TOP_K
    token_table = jnp.zeros((EXPERTS, sources * CAP), jnp.int32).at[flat_routes, column].set(token_index)
    weight_table = jnp.zeros((EXPERTS, sources * CAP), jnp.float32).at[flat_routes, column].set(routing_weight.reshape(sources, assigned))
    half_width = FE // N_TP

    def per_expert(total, expert_pieces):
        tokens_here, weights_here, gate_here, up_here, down_here = expert_pieces
        picked = normed[tokens_here]
        gate_part = jnp.dot(picked, gate_here, preferred_element_type=jnp.float32)
        up_part = jnp.dot(picked, up_here, preferred_element_type=jnp.float32)
        inner = (jax.nn.silu(gate_part) * up_part).astype(jnp.bfloat16)
        expert_sum = jnp.zeros((picked.shape[0], D), jnp.float32)
        for group in range(N_TP):
            expert_sum = expert_sum + round_half(jnp.dot(inner[:, group * half_width:(group + 1) * half_width], down_here[group * half_width:(group + 1) * half_width], preferred_element_type=jnp.float32))
        expert_result = round_half(expert_sum)
        return (total.at[tokens_here].add(weights_here[:, None] * expert_result), None)
    routed, _ = lax.scan(per_expert, jnp.zeros((token_count, D), jnp.float32), (token_table, weight_table, routed_gate_weight, routed_up_weight, routed_down_weight))
    shared_gate_out = jnp.dot(normed, common_gate_weight, preferred_element_type=jnp.float32)
    shared_up_out = jnp.dot(normed, common_up_weight, preferred_element_type=jnp.float32)
    shared_inner = (jax.nn.silu(shared_gate_out) * shared_up_out).astype(jnp.bfloat16)
    feed = jnp.dot(shared_inner, common_down_weight, preferred_element_type=jnp.float32) + routed
    return layer_norm(normed.astype(jnp.float32) + feed, final_norm_gain).astype(jnp.bfloat16)
```

```python
import jax
import jax.numpy as jnp
from jax import lax
from jax.experimental import pallas as pl
from jax.experimental.pallas import tpu as pltpu
from jax.sharding import PartitionSpec as P

F32 = jnp.float32
BF16 = jnp.bfloat16
MESH = pl.DeviceIdType.MESH
EPS = 1e-06
SP_TP = ("sp", "tp")

N_SP = 64
TOK = 256
ROWS = 128
PAIRS = 8
WIDE = 2048
CHUNKS = 4
PER = N_SP // CHUNKS
CAP = 8
MIX = 27


def dot(a, b):
    return jnp.dot(a, b, preferred_element_type=F32)


def dot_nt(a, b):
    return lax.dot_general(a, b, (((1,), (1,)), ((), ())), preferred_element_type=F32)


def dot_tn(a, b):
    return lax.dot_general(a, b, (((0,), (0,)), ((), ())), preferred_element_type=F32)


def split3(x):
    hi = x.astype(BF16)
    rest = x - hi.astype(F32)
    mid = rest.astype(BF16)
    return hi, mid, (rest - mid.astype(F32)).astype(BF16)


def offset_of(i):
    return (i * MIX) & (N_SP - 1)


def shifted(me, s, sign):
    z = ((me >> 4) + sign * (s >> 4)) & 3
    y = (((me >> 2) & 3) + sign * ((s >> 2) & 3)) & 3
    x = ((me & 3) + sign * (s & 3)) & 3
    return z * 16 + y * 4 + x


def silu(x):
    return x / (1.0 + jnp.exp(-x))


def log_sigmoid(x):
    t = jnp.exp(-jnp.abs(x))
    return jnp.minimum(x, 0.0) - jnp.log1p(t)


def lanes(p, width=128):
    return pl.ds(pl.multiple_of(p * width, width), width)


def iota(shape, axis):
    return lax.broadcasted_iota(jnp.int32, shape, axis)


def layer_kernel(
    q_hbm, k_hbm, v_hbm, g_hbm, a_hbm, x_hbm, res_hbm, hgain_ref, wo_hbm, mgain_ref,
    routes_ref, rw_ref, wg_hbm, wu_hbm, wd_hbm, cg_hbm, cu_hbm, cd_hbm, fgain_ref,
    out_ref,
    q_s, k_s, v_s, g_s, a_s, x_s, res_s, wo_s, cg_s, cu_s, cd_s, wg_s, wu_s, wd_s,
    from_s, local_s, qcat_s, st_out, st_in, tot_out, tot_in, sc_out, inc_s,
    gated_s, own_s, pr_out, pr_in, normed_s, pick_s, comb_s,
    dsp_out, dsp_in, xb_s, inner_s, e_out, ret_s, acc_s,
    ld_sem, w_own_sem, w_send, w_recv, st_send, st_recv, tt_send, tt_recv, sc_send, sc_recv,
    pr_send, pr_recv, d_send, d_recv, r_send, r_recv,
):
    me = lax.axis_index("sp")
    core = lax.axis_index("tp")
    other = 1 - core

    sources = (a_hbm, x_hbm, k_hbm, v_hbm, q_hbm, g_hbm, wo_hbm, res_hbm, cg_hbm, cu_hbm, cd_hbm)
    targets = (a_s, x_s, k_s, v_s, q_s, g_s, wo_s, res_s, cg_s, cu_s, cd_s)
    loads = [
        pltpu.make_async_copy(s, t, ld_sem.at[i]) for i, (s, t) in enumerate(zip(sources, targets))
    ]
    for load in loads[:6]:
        load.start()

    barrier = pltpu.get_barrier_semaphore()

    def greet(s, carry):
        pl.semaphore_signal(
            barrier, inc=1, device_id={"sp": shifted(me, s, 1)}, device_id_type=MESH
        )
        return carry

    lax.fori_loop(1, N_SP, greet, 0)
    pl.semaphore_signal(barrier, inc=1, device_id={"tp": other}, device_id_type=MESH)

    low = iota((TOK, TOK), 0) >= iota((TOK, TOK), 1)
    low_bf = jnp.where(low, 1.0, 0.0).astype(BF16)
    half64 = iota((64, 128), 1) < 64
    for load in loads[:4]:
        load.wait()

    def own_state(p, carry):
        decay = log_sigmoid(a_s[:, lanes(p)].astype(F32)) * (1.0 / 16.0)
        spread = jnp.where(iota((16, 128), 0) == 2 * p + (iota((16, 128), 1) >> 6), 1.0, 0.0)
        spread = spread.astype(BF16)
        for part in split3(x_s[...]):
            decay = decay + dot(part, spread)
        hi, mid, lo = split3(decay)
        total = dot(low_bf, hi) + dot(low_bf, mid) + dot(low_bf, lo)
        from_s[:, lanes(p)] = total
        last = total[TOK - 1 :, :]
        tot_out[p] = jnp.exp(last)
        key = k_s[:, lanes(p)].astype(F32)
        up = (key * jnp.exp(total)).astype(BF16)
        end = (key * jnp.exp(last - total)).astype(BF16)
        value = v_s[:, lanes(p)]
        left = dot_tn(value, end)
        right = dot_tn(value, up)
        left = jnp.where(half64, left[:64], left[64:]).astype(BF16)
        right = jnp.where(half64, right[:64], right[64:]).astype(BF16)
        for part in range(4):
            st_out[4 * p + part] = left[16 * part : 16 * part + 16]
            st_out[32 + 4 * p + part] = right[16 * part : 16 * part + 16]
        return carry

    lax.fori_loop(0, PAIRS, own_state, 0)

    pl.semaphore_wait(barrier, N_SP)

    def send_state(i, carry):
        to = shifted(me, offset_of(i), 1)
        pltpu.make_async_remote_copy(
            st_out.at[to], st_in.at[me], st_send, st_recv,
            device_id={"sp": to}, device_id_type=MESH,
        ).start()
        pltpu.make_async_remote_copy(
            tot_out.at[(to & 31) >> 2], tot_in.at[me], tt_send, tt_recv,
            device_id={"sp": to}, device_id_type=MESH,
        ).start()
        return carry

    lax.fori_loop(1, N_SP, send_state, 0)
    for load in loads[6:]:
        load.start()
    w_pairs = ((wg_hbm, wg_s), (wu_hbm, wu_s), (wd_hbm, wd_s))
    own_w = [
        pltpu.make_async_copy(s.at[0], t.at[0], w_own_sem.at[i]) for i, (s, t) in enumerate(w_pairs)
    ]
    far_w = [
        pltpu.make_async_remote_copy(
            s.at[0], t.at[1], w_send.at[i], w_recv.at[i],
            device_id={"tp": other}, device_id_type=MESH,
        )
        for i, (s, t) in enumerate(w_pairs)
    ]
    for copy in own_w + far_w:
        copy.start()
    st_in[me] = st_out[me]
    tot_in[me] = tot_out[(me & 31) >> 2]

    loads[4].wait()
    even = iota((ROWS, 128), 1) < 64
    ahead_mask = iota((ROWS, 256), 0) >= (iota((ROWS, 256), 1) & (ROWS - 1))
    zero = jnp.zeros((ROWS, 128), BF16)

    def both(x):
        return jnp.concatenate([jnp.where(even, x, zero), jnp.where(even, zero, x)], axis=0)

    def local_pair(p, carry):
        total = from_s[:, lanes(p)]
        query = q_s[:, lanes(p)].astype(F32) * 0.125
        key = k_s[:, lanes(p)].astype(F32)
        value = v_s[:, lanes(p)]
        last = total[TOK - 1 :, :]
        qcat_s[:, pl.ds(pl.multiple_of(p * 256, 256), 128)] = (query * jnp.exp(total)).astype(BF16)
        qcat_s[:, pl.ds(pl.multiple_of(p * 256 + 128, 128), 128)] = (
            query * jnp.exp(last - total)
        ).astype(BF16)
        mid_total = total[ROWS - 1 : ROWS, :]
        across = jnp.exp(-jnp.abs(total - mid_total))
        query_across = (query * across).astype(BF16)
        key_across = (key * across).astype(BF16)
        for b in range(2):
            rows = slice(ROWS * b, ROWS * b + ROWS)
            far = slice(ROWS * (1 - b), ROWS * (1 - b) + ROWS)
            center = total[rows] - total[ROWS * b + 63 : ROWS * b + 64, :]
            grow = jnp.exp(center)
            fade = jnp.exp(-center)
            ahead = dot_nt((query[rows] * grow).astype(BF16), both((key[rows] * fade).astype(BF16)))
            behind = dot_nt(
                (query[rows] * fade).astype(BF16), both((key[rows] * grow).astype(BF16))
            )
            scores = jnp.where(ahead_mask, ahead, behind).astype(BF16)
            result = dot(scores, both(value[rows]))
            state = dot_tn(value[far], key_across[far])
            state = jnp.where((iota((128, 128), 0) < 64) == even, state, 0.0).astype(BF16)
            result = result + dot_nt(query_across[rows], state)
            local_s[rows, lanes(p)] = result
        return carry

    lax.fori_loop(0, PAIRS, local_pair, 0)

    lane = iota((ROWS, N_SP * CAP), 1)
    expert = shifted(me, offset_of(lane >> 3), 1)
    first = routes_ref[:, 0:1] == expert
    second = routes_ref[:, 1:2] == expert
    named = jnp.where(first | second, 1.0, 0.0)
    strict = jnp.where(iota((ROWS, ROWS), 0) > iota((ROWS, ROWS), 1), 1.0, 0.0).astype(BF16)
    rank = dot(strict, named.astype(BF16))
    chosen = (named > 0.5) & (rank == (lane & (CAP - 1)).astype(F32))
    pick = jnp.where(chosen, 1.0, 0.0).astype(BF16)
    weight = jnp.where(chosen, jnp.where(first, rw_ref[:, 0:1], rw_ref[:, 1:2]), 0.0)
    weight_hi = weight.astype(BF16)
    weight_lo = (weight - weight_hi.astype(F32)).astype(BF16)
    for c in range(CHUNKS):
        part = slice(ROWS * c, ROWS * c + ROWS)
        pick_s[c] = pick[:, part]
        comb_s[c, :ROWS] = weight_hi[:, part]
        comb_s[c, ROWS:] = weight_lo[:, part]

    def drain(buffer, count, send, recv):
        done = pltpu.make_async_remote_copy(
            buffer.at[pl.ds(0, count)], buffer.at[pl.ds(0, count)], send, recv,
            device_id={"tp": other}, device_id_type=MESH,
        )
        return done

    drain(st_in, N_SP - 1, st_send, st_recv).wait_recv()
    drain(tot_in, N_SP - 1, tt_send, tt_recv).wait_recv()
    backward = me >= 32

    def scan_step(i, state):
        at = jnp.where(backward, N_SP - 1 - i, i)
        sc_out[at] = state.astype(BF16)
        return state * tot_in[at] + st_in[at].astype(F32)

    lax.fori_loop(0, N_SP, scan_step, jnp.zeros((16, 128), F32), unroll=4)

    def send_scan(i, carry):
        to = shifted(me, offset_of(i), 1)
        pltpu.make_async_remote_copy(
            sc_out.at[to], inc_s.at[me], sc_send, sc_recv,
            device_id={"sp": to}, device_id_type=MESH,
        ).start()
        return carry

    lax.fori_loop(1, N_SP, send_scan, 0)
    inc_s[me] = sc_out[me]
    loads[5].wait()
    loads[6].wait()
    loads[7].wait()
    drain(inc_s, N_SP - 1, sc_send, sc_recv).wait_recv()

    block_mean = jnp.where((iota((128, 128), 0) < 64) == even, 1.0 / 64.0, 0.0).astype(BF16)
    gain = jnp.concatenate([hgain_ref[...], hgain_ref[...]], axis=1)
    hzero = jnp.zeros((64, 128), BF16)

    def mix_pair(p, carry):
        left = jnp.concatenate([inc_s[4 * p + part] for part in range(4)], axis=0)
        right = jnp.concatenate([inc_s[32 + 4 * p + part] for part in range(4)], axis=0)
        state = jnp.concatenate(
            [
                jnp.concatenate([jnp.where(half64, left, hzero), jnp.where(half64, right, hzero)], axis=1),
                jnp.concatenate([jnp.where(half64, hzero, left), jnp.where(half64, hzero, right)], axis=1),
            ],
            axis=0,
        )
        mixed = local_s[:, lanes(p)] + dot_nt(qcat_s[:, lanes(p, 256)], state)
        square = mixed * mixed
        square_hi = square.astype(BF16)
        square_lo = (square - square_hi.astype(F32)).astype(BF16)
        mean = dot(square_hi, block_mean) + dot(square_lo, block_mean)
        gate = silu(g_s[:, lanes(p)].astype(F32))
        gated_s[:, lanes(p)] = (mixed * lax.rsqrt(mean + EPS) * gain * gate).astype(BF16)
        return carry

    lax.fori_loop(0, PAIRS, mix_pair, 0)

    def send_partial(n):
        return pltpu.make_async_remote_copy(
            pr_out.at[n], pr_in.at[n], pr_send.at[n], pr_recv.at[n],
            device_id={"tp": other}, device_id_type=MESH,
        )

    def project(n, carry):
        part = dot(gated_s[...], wo_s[:, lanes(n, 512)]).astype(BF16)
        mine, theirs = part[:ROWS], part[ROWS:]
        own_s[:, lanes(n, 512)] = jnp.where(core == 0, mine, theirs)
        pr_out[n] = jnp.where(core == 0, theirs, mine)
        send_partial(n).start()
        return carry

    lax.fori_loop(0, 4, project, 0)

    def residual_sum(n, total):
        send_partial(n).wait_recv()
        r = res_s[:, lanes(n, 512)].astype(F32) + (
            own_s[:, lanes(n, 512)].astype(F32) + pr_in[n].astype(F32)
        )
        acc_s[:, lanes(n, 512)] = r
        return total + jnp.sum(r, axis=1, keepdims=True)

    def norm_to(target, gain_ref, total):
        mean = total * (1.0 / WIDE)

        def spread(n, s):
            d = acc_s[:, lanes(n, 512)] - mean
            return s + jnp.sum(d * d, axis=1, keepdims=True)

        var = lax.fori_loop(0, 4, spread, jnp.zeros((ROWS, 1), F32)) * (1.0 / WIDE)
        scale = lax.rsqrt(var + EPS)

        def write(n, carry):
            d = acc_s[:, lanes(n, 512)] - mean
            target[:, lanes(n, 512)] = (d * scale * gain_ref[:, lanes(n, 512)]).astype(BF16)
            return carry

        lax.fori_loop(0, 4, write, 0)

    norm_to(
        normed_s, mgain_ref, lax.fori_loop(0, 4, residual_sum, jnp.zeros((ROWS, 1), F32))
    )

    def dispatch(c, carry):
        for n in range(4):
            rows = dot_tn(pick_s[c], normed_s[:, 512 * n : 512 * n + 512])
            dsp_out[pl.ds(c * PER, PER), :, 512 * n : 512 * n + 512] = rows.reshape(
                PER, CAP, 512
            ).astype(BF16)

        def send(j, carry):
            i = c * PER + j

            @pl.when(i > 0)
            def _():
                pltpu.make_async_remote_copy(
                    dsp_out.at[i], dsp_in.at[i], d_send, d_recv.at[c],
                    device_id={"sp": shifted(me, offset_of(i), 1)}, device_id_type=MESH,
                ).start()

            return carry

        lax.fori_loop(0, PER, send, 0)
        return carry

    lax.fori_loop(0, CHUNKS, dispatch, 0)
    dsp_in[0] = dsp_out[0]

    for load in loads[8:]:
        load.wait()

    def shared_inner(n, carry):
        gate = dot(normed_s[...], cg_s[:, lanes(n, 256)])
        up = dot(normed_s[...], cu_s[:, lanes(n, 256)])
        inner_s[:, lanes(n, 256)] = (silu(gate) * up).astype(BF16)
        return carry

    lax.fori_loop(0, 2, shared_inner, 0)

    def shared_down(n, carry):
        down = dot(inner_s[:, 0:512], cd_s[:, lanes(n, 512)])
        acc_s[:, lanes(n, 512)] = normed_s[:, lanes(n, 512)].astype(F32) + down
        return carry

    lax.fori_loop(0, 4, shared_down, 0)

    for copy in own_w:
        copy.wait()
    for copy in far_w:
        copy.wait()

    def expert_chunk(c, first):
        xb_s[...] = dsp_in[pl.ds(c * PER, PER)].astype(F32).reshape(ROWS, WIDE).astype(BF16)

        def inner(t, carry):
            h, n = t >> 1, t & 1
            gate = dot(xb_s[...], wg_s[h, :, lanes(n, 256)])
            up = dot(xb_s[...], wu_s[h, :, lanes(n, 256)])
            inner_s[:, lanes(t, 256)] = (silu(gate) * up).astype(BF16)
            return carry

        lax.fori_loop(0, 4, inner, 0)

        def down(n, carry):
            result = dot(inner_s[:, 0:512], wd_s[0, :, lanes(n, 512)])
            result = result + dot(inner_s[:, 512:1024], wd_s[1, :, lanes(n, 512)])
            e_out[pl.ds(c * PER, PER), :, lanes(n, 512)] = result.reshape(PER, CAP, 512).astype(BF16)
            return carry

        lax.fori_loop(0, 4, down, 0)

        def send(j, carry):
            i = c * PER + j

            @pl.when(i > 0)
            def _():
                pltpu.make_async_remote_copy(
                    e_out.at[i], ret_s.at[i], r_send, r_recv.at[c],
                    device_id={"sp": shifted(me, offset_of(i), -1)}, device_id_type=MESH,
                ).start()

            return carry

        lax.fori_loop(0, PER, send, 0)

    def arrived(buffer, c, recv):
        def wait(count):
            pltpu.make_async_remote_copy(
                buffer.at[pl.ds(0, count)], buffer.at[pl.ds(0, count)], d_send, recv.at[c],
                device_id={"tp": other}, device_id_type=MESH,
            ).wait_recv()

        @pl.when(c == 0)
        def _():
            wait(PER - 1)

        @pl.when(c > 0)
        def _():
            wait(PER)

    def experts(c, carry):
        arrived(dsp_in, c, d_recv)
        expert_chunk(c, 0)
        return carry

    lax.fori_loop(0, CHUNKS, experts, 0)
    ret_s[0] = e_out[0]

    def combine(c, carry):
        arrived(ret_s, c, r_recv)

        def part(n, carry):
            rows = ret_s[pl.ds(c * PER, PER), :, lanes(n, 512)]
            rows = rows.astype(F32).reshape(ROWS, 512).astype(BF16)
            both_parts = dot(comb_s[c], rows)
            acc_s[:, lanes(n, 512)] += both_parts[:ROWS] + both_parts[ROWS:]
            return carry

        lax.fori_loop(0, 4, part, 0)
        return carry

    lax.fori_loop(0, CHUNKS, combine, 0)

    def total_of(n, total):
        return total + jnp.sum(acc_s[:, lanes(n, 512)], axis=1, keepdims=True)

    norm_to(out_ref, fgain_ref, lax.fori_loop(0, 4, total_of, jnp.zeros((ROWS, 1), F32)))

    drain(st_in, N_SP - 1, st_send, st_recv).wait_send()
    drain(tot_in, N_SP - 1, tt_send, tt_recv).wait_send()
    drain(inc_s, N_SP - 1, sc_send, sc_recv).wait_send()
    drain(dsp_in, N_SP - 1, d_send, d_recv.at[0]).wait_send()
    drain(ret_s, N_SP - 1, r_send, r_recv.at[0]).wait_send()

    def partial_left(n, carry):
        send_partial(n).wait_send()
        return carry

    lax.fori_loop(0, 4, partial_left, 0)


def per_device(
    q, k, v, g, a, x, res, hgain, wo, mgain, routes, rw, wg, wu, wd, cg, cu, cd, fgain
):
    anywhere = pl.BlockSpec(memory_space=pl.ANY)
    vmem = pl.BlockSpec(memory_space=pltpu.VMEM)
    specs = [anywhere] * 7 + [vmem, anywhere, vmem, vmem, vmem] + [anywhere] * 6 + [vmem]
    dma = pltpu.SemaphoreType.DMA
    scratch = [
        pltpu.VMEM((TOK, 1024), BF16),
        pltpu.VMEM((TOK, 1024), BF16),
        pltpu.VMEM((TOK, 1024), BF16),
        pltpu.VMEM((TOK, 1024), BF16),
        pltpu.VMEM((TOK, 1024), BF16),
        pltpu.VMEM((TOK, 16), F32),
        pltpu.VMEM((ROWS, WIDE), BF16),
        pltpu.VMEM((1024, WIDE), BF16),
        pltpu.VMEM((WIDE, 512), BF16),
        pltpu.VMEM((WIDE, 512), BF16),
        pltpu.VMEM((512, WIDE), BF16),
        pltpu.VMEM((2, WIDE, 512), BF16),
        pltpu.VMEM((2, WIDE, 512), BF16),
        pltpu.VMEM((2, 512, WIDE), BF16),
        pltpu.VMEM((TOK, 1024), F32),
        pltpu.VMEM((TOK, 1024), F32),
        pltpu.VMEM((TOK, WIDE), BF16),
        pltpu.VMEM((N_SP, 16, 128), BF16),
        pltpu.VMEM((N_SP, 16, 128), BF16),
        pltpu.VMEM((PAIRS, 1, 128), F32),
        pltpu.VMEM((N_SP, 1, 128), F32),
        pltpu.VMEM((N_SP, 16, 128), BF16),
        pltpu.VMEM((N_SP, 16, 128), BF16),
        pltpu.VMEM((TOK, 1024), BF16),
        pltpu.VMEM((ROWS, WIDE), BF16),
        pltpu.VMEM((4, ROWS, 512), BF16),
        pltpu.VMEM((4, ROWS, 512), BF16),
        pltpu.VMEM((ROWS, WIDE), BF16),
        pltpu.VMEM((CHUNKS, ROWS, ROWS), BF16),
        pltpu.VMEM((CHUNKS, 2 * ROWS, ROWS), BF16),
        pltpu.VMEM((N_SP, CAP, WIDE), BF16),
        pltpu.VMEM((N_SP, CAP, WIDE), BF16),
        pltpu.VMEM((ROWS, WIDE), BF16),
        pltpu.VMEM((ROWS, 1024), BF16),
        pltpu.VMEM((N_SP, CAP, WIDE), BF16),
        pltpu.VMEM((N_SP, CAP, WIDE), BF16),
        pltpu.VMEM((ROWS, WIDE), F32),
        dma((11,)), dma((3,)), dma((3,)), dma((3,)),
        dma, dma, dma, dma, dma, dma,
        dma((4,)), dma((4,)),
        dma, dma((CHUNKS,)), dma, dma((CHUNKS,)),
    ]
    return pl.pallas_call(
        layer_kernel,
        name="layer",
        out_shape=jax.ShapeDtypeStruct((ROWS, WIDE), BF16),
        in_specs=specs,
        out_specs=vmem,
        scratch_shapes=scratch,
        compiler_params=pltpu.CompilerParams(
            collective_id=0, has_side_effects=True, vmem_limit_bytes=60 * 1024 * 1024
        ),
    )(
        q, k, v, g, a, x, res, hgain.reshape(1, -1), wo, mgain.reshape(1, -1), routes, rw,
        wg, wu, wd, cg, cu, cd, fgain.reshape(1, -1),
    )


def solution(mesh):
    return jax.shard_map(
        per_device,
        mesh=mesh,
        in_specs=(
            P("sp", "tp"),
            P("sp", "tp"),
            P("sp", "tp"),
            P("sp", "tp"),
            P("sp", "tp"),
            P("sp", "tp"),
            P(SP_TP, None),
            P(),
            P("tp", None),
            P(),
            P(SP_TP, None),
            P(SP_TP, None),
            P("sp", None, "tp"),
            P("sp", None, "tp"),
            P("sp", "tp", None),
            P(),
            P(),
            P(),
            P(),
        ),
        out_specs=P(SP_TP, None),
        check_vma=False,
    )
```

```python
import jax
import jax.numpy as jnp
from jax import lax
from jax.experimental import pallas as pl
from jax.experimental.pallas import tpu as pltpu
from jax.sharding import PartitionSpec as P

F32 = jnp.float32
BF16 = jnp.bfloat16
MESH = pl.DeviceIdType.MESH
EPS = 1e-06
SP_TP = ("sp", "tp")

N_SP = 64
TOK = 256
ROWS = 128
PAIRS = 8
WIDE = 2048
CHUNKS = 4
PER = N_SP // CHUNKS
CAP = 8


def hops(s):
    return sum(min(d, 4 - d) for d in (s >> 4, (s >> 2) & 3, s & 3))


FAR_FIRST = sorted(range(1, N_SP), key=lambda s: -hops(s))
SLOTS = [27 * i % N_SP for i in range(N_SP)]


def dot(a, b):
    return jnp.dot(a, b, preferred_element_type=F32)


def dot_nt(a, b):
    return lax.dot_general(a, b, (((1,), (1,)), ((), ())), preferred_element_type=F32)


def dot_tn(a, b):
    return lax.dot_general(a, b, (((0,), (0,)), ((), ())), preferred_element_type=F32)


def split2(x):
    hi = x.astype(BF16)
    return hi, (x - hi.astype(F32)).astype(BF16)


def shifted(me, s, sign):
    z = ((me >> 4) + sign * (s >> 4)) & 3
    y = (((me >> 2) & 3) + sign * ((s >> 2) & 3)) & 3
    x = ((me & 3) + sign * (s & 3)) & 3
    return z * 16 + y * 4 + x


def silu(x):
    return x / (1.0 + jnp.exp(-x))


def log_sigmoid(x):
    return jnp.minimum(x, 0.0) - jnp.log(1.0 + jnp.exp(-jnp.abs(x)))


def lanes(p, width=128):
    return pl.ds(pl.multiple_of(p * width, width), width)


def iota(shape, axis):
    return lax.broadcasted_iota(jnp.int32, shape, axis)


def layer_kernel(
    q_hbm, k_hbm, v_hbm, g_hbm, a_hbm, x_hbm, res_hbm, hgain_ref, wo_hbm, mgain_ref,
    routes_ref, rw_ref, wg_hbm, wu_hbm, wd_hbm, cg_hbm, cu_hbm, cd_hbm, fgain_ref,
    out_ref,
    q_s, k_s, v_s, g_s, a_s, x_s, res_s, wo_s, cg_s, cu_s, cd_s, wg_s, wu_s, wd_s,
    from_s, local_s, qcat_s, st_out, st_in, tot_out, tot_in, sc_out, inc_s,
    gate_s, gated_s, own_s, pr_out, pr_in, normed_s, pick_s, comb_s,
    dsp_out, dsp_in, xb_s, inner_s, e_out, ret_s, acc_s,
    ld_sem, w_own_sem, w_send, w_recv, st_send, st_recv, tt_send, tt_recv, sc_send, sc_recv,
    pr_send, pr_recv, d_send, d_recv, r_send, r_recv,
):
    me = lax.axis_index("sp")
    core = lax.axis_index("tp")
    other = 1 - core

    sources = (a_hbm, x_hbm, k_hbm, v_hbm, q_hbm, g_hbm, wo_hbm, res_hbm, cg_hbm, cu_hbm, cd_hbm)
    targets = (a_s, x_s, k_s, v_s, q_s, g_s, wo_s, res_s, cg_s, cu_s, cd_s)
    loads = [
        pltpu.make_async_copy(s, t, ld_sem.at[i]) for i, (s, t) in enumerate(zip(sources, targets))
    ]
    for load in loads[:6]:
        load.start()

    barrier = pltpu.get_barrier_semaphore()

    for s in FAR_FIRST:
        pl.semaphore_signal(
            barrier, inc=1, device_id={"sp": shifted(me, s, 1)}, device_id_type=MESH
        )
    pl.semaphore_signal(barrier, inc=1, device_id={"tp": other}, device_id_type=MESH)

    low = iota((TOK, TOK), 0) >= iota((TOK, TOK), 1)
    low_bf = jnp.where(low, 1.0, 0.0).astype(BF16)
    half64 = iota((64, 128), 1) < 64
    for load in loads[:4]:
        load.wait()
    w_pairs = ((wg_hbm, wg_s), (wu_hbm, wu_s), (wd_hbm, wd_s))
    own_w = [
        pltpu.make_async_copy(s.at[0], t.at[0], w_own_sem.at[i]) for i, (s, t) in enumerate(w_pairs)
    ]
    far_w = [
        pltpu.make_async_remote_copy(
            s.at[0], t.at[1], w_send.at[i], w_recv.at[i],
            device_id={"tp": other}, device_id_type=MESH,
        )
        for i, (s, t) in enumerate(w_pairs)
    ]
    for load in loads[6:] + own_w:
        load.start()

    added_hi = x_s[...].astype(BF16)
    rest = x_s[...] - added_hi.astype(F32)
    added = jnp.concatenate([added_hi.astype(F32)] + [r.astype(F32) for r in split2(rest)], axis=0)
    added = added.T.astype(BF16)

    def own_state(p, carry):
        spread = jnp.where((iota((48, 128), 0) & 15) == 2 * p + (iota((48, 128), 1) >> 6), 1.0, 0.0)
        decay = log_sigmoid(a_s[:, lanes(p)].astype(F32)) * (1.0 / 16.0)
        decay = decay + dot(added, spread.astype(BF16))
        summed = dot(low_bf, jnp.concatenate(split2(decay), axis=1))
        total = summed[:, :128] + summed[:, 128:]
        from_s[:, lanes(p)] = total
        last = total[TOK - 1 :, :]
        tot_out[p] = jnp.exp(last)
        key = k_s[:, lanes(p)].astype(F32)
        up = (key * jnp.exp(total)).astype(BF16)
        end = (key * jnp.exp(last - total)).astype(BF16)
        state = dot_tn(v_s[:, lanes(p)], jnp.concatenate([end, up], axis=1))
        left = jnp.where(half64, state[:64, :128], state[64:, :128]).astype(BF16)
        right = jnp.where(half64, state[:64, 128:], state[64:, 128:]).astype(BF16)
        for part in range(4):
            st_out[4 * p + part] = left[16 * part : 16 * part + 16]
            st_out[32 + 4 * p + part] = right[16 * part : 16 * part + 16]
        return carry

    lax.fori_loop(0, PAIRS, own_state, 0, unroll=2)

    pl.semaphore_wait(barrier, N_SP)

    for s in FAR_FIRST:
        to = shifted(me, s, 1)
        pltpu.make_async_remote_copy(
            st_out.at[to], st_in.at[me], st_send, st_recv,
            device_id={"sp": to}, device_id_type=MESH,
        ).start()
        pltpu.make_async_remote_copy(
            tot_out.at[(to & 31) >> 2], tot_in.at[me], tt_send, tt_recv,
            device_id={"sp": to}, device_id_type=MESH,
        ).start()
    st_in[me] = st_out[me]
    tot_in[me] = tot_out[(me & 31) >> 2]

    loads[4].wait()
    even = iota((ROWS, 128), 1) < 64
    ahead_mask = iota((ROWS, 256), 0) >= (iota((ROWS, 256), 1) & (ROWS - 1))
    zero = jnp.zeros((ROWS, 128), BF16)

    def both(x):
        return jnp.concatenate([jnp.where(even, x, zero), jnp.where(even, zero, x)], axis=0)

    def local_pair(p, carry):
        total = from_s[:, lanes(p)]
        query = q_s[:, lanes(p)].astype(F32) * 0.125
        key = k_s[:, lanes(p)].astype(F32)
        value = v_s[:, lanes(p)]
        last = total[TOK - 1 :, :]
        qcat_s[:, pl.ds(pl.multiple_of(p * 256, 256), 128)] = (query * jnp.exp(total)).astype(BF16)
        qcat_s[:, pl.ds(pl.multiple_of(p * 256 + 128, 128), 128)] = (
            query * jnp.exp(last - total)
        ).astype(BF16)
        mid_total = total[ROWS - 1 : ROWS, :]
        across = jnp.exp(-jnp.abs(total - mid_total))
        query_across = (query * across).astype(BF16)
        key_across = (key * across).astype(BF16)
        for b in range(2):
            rows = slice(ROWS * b, ROWS * b + ROWS)
            far = slice(ROWS * (1 - b), ROWS * (1 - b) + ROWS)
            center = total[rows] - total[ROWS * b + 63 : ROWS * b + 64, :]
            grow = jnp.exp(center)
            fade = jnp.exp(-center)
            ahead = dot_nt((query[rows] * grow).astype(BF16), both((key[rows] * fade).astype(BF16)))
            behind = dot_nt(
                (query[rows] * fade).astype(BF16), both((key[rows] * grow).astype(BF16))
            )
            scores = jnp.where(ahead_mask, ahead, behind).astype(BF16)
            result = dot(scores, both(value[rows]))
            state = dot_tn(value[far], key_across[far])
            state = jnp.where((iota((128, 128), 0) < 64) == even, state, 0.0).astype(BF16)
            result = result + dot_nt(query_across[rows], state)
            local_s[rows, lanes(p)] = result
        return carry

    lax.fori_loop(0, PAIRS // 2, local_pair, 0)

    strict = jnp.where(iota((ROWS, ROWS), 0) < iota((ROWS, ROWS), 1), 1.0, 0.0).astype(BF16)
    slot = iota((ROWS, ROWS), 0)

    for c in range(CHUNKS):
        expert = jnp.concatenate(
            [
                jnp.full((CAP, ROWS), shifted(me, s, 1), jnp.int32)
                for s in SLOTS[PER * c : PER * c + PER]
            ],
            axis=0,
        )
        first = routes_ref[0:1, :] == expert
        second = routes_ref[1:2, :] == expert
        named = jnp.where(first | second, 1.0, 0.0)
        rank = dot(named.astype(BF16), strict)
        chosen = (named > 0.5) & (rank == (slot & (CAP - 1)).astype(F32))
        pick_s[c] = jnp.where(chosen, 1.0, 0.0).astype(BF16)
        weight = jnp.where(chosen, jnp.where(first, rw_ref[0:1, :], rw_ref[1:2, :]), 0.0).T
        weight_hi = weight.astype(BF16)
        comb_s[c, :ROWS] = weight_hi
        comb_s[c, ROWS:] = (weight - weight_hi.astype(F32)).astype(BF16)

    def drain(buffer, count, send, recv):
        done = pltpu.make_async_remote_copy(
            buffer.at[pl.ds(0, count)], buffer.at[pl.ds(0, count)], send, recv,
            device_id={"tp": other}, device_id_type=MESH,
        )
        return done

    drain(st_in, N_SP - 1, st_send, st_recv).wait_recv()
    drain(tot_in, N_SP - 1, tt_send, tt_recv).wait_recv()
    backward = me >= 32

    def scan_step(i, state):
        at = jnp.where(backward, N_SP - 1 - i, i)
        sc_out[at] = state.astype(BF16)
        return state * tot_in[at] + st_in[at].astype(F32)

    lax.fori_loop(0, N_SP, scan_step, jnp.zeros((16, 128), F32), unroll=16)

    for s in FAR_FIRST:
        to = shifted(me, s, 1)
        pltpu.make_async_remote_copy(
            sc_out.at[to], inc_s.at[me], sc_send, sc_recv,
            device_id={"sp": to}, device_id_type=MESH,
        ).start()
    inc_s[me] = sc_out[me]
    lax.fori_loop(PAIRS // 2, PAIRS, local_pair, 0)
    loads[5].wait()
    gain = jnp.concatenate([hgain_ref[...], hgain_ref[...]], axis=1)

    def gates(p, carry):
        gate_s[:, lanes(p)] = silu(g_s[:, lanes(p)].astype(F32)) * gain
        return carry

    lax.fori_loop(0, PAIRS, gates, 0)
    loads[6].wait()
    loads[7].wait()
    drain(inc_s, N_SP - 1, sc_send, sc_recv).wait_recv()

    block_mean = jnp.where(
        ((iota((TOK, 128), 0) >> 6) & 1) == (iota((TOK, 128), 1) >> 6), 1.0 / 64.0, 0.0
    ).astype(BF16)
    hzero = jnp.zeros((64, 128), BF16)

    def mix_pair(p, carry):
        left = jnp.concatenate([inc_s[4 * p + part] for part in range(4)], axis=0)
        right = jnp.concatenate([inc_s[32 + 4 * p + part] for part in range(4)], axis=0)
        state = jnp.concatenate(
            [
                jnp.concatenate([jnp.where(half64, left, hzero), jnp.where(half64, right, hzero)], axis=1),
                jnp.concatenate([jnp.where(half64, hzero, left), jnp.where(half64, hzero, right)], axis=1),
            ],
            axis=0,
        )
        mixed = local_s[:, lanes(p)] + dot_nt(qcat_s[:, lanes(p, 256)], state)
        mean = dot(jnp.concatenate(split2(mixed * mixed), axis=1), block_mean)
        gated_s[:, lanes(p)] = (mixed * lax.rsqrt(mean + EPS) * gate_s[:, lanes(p)]).astype(BF16)
        return carry

    lax.fori_loop(0, PAIRS, mix_pair, 0, unroll=4)

    def send_partial(n):
        return pltpu.make_async_remote_copy(
            pr_out.at[n], pr_in.at[n], pr_send.at[n], pr_recv.at[n],
            device_id={"tp": other}, device_id_type=MESH,
        )

    def project(n, carry):
        part = dot(gated_s[...], wo_s[:, lanes(n, 512)]).astype(BF16)
        mine, theirs = part[:ROWS], part[ROWS:]
        own_s[:, lanes(n, 512)] = jnp.where(core == 0, mine, theirs)
        pr_out[n] = jnp.where(core == 0, theirs, mine)
        send_partial(n).start()
        return carry

    lax.fori_loop(0, 4, project, 0, unroll=True)

    def residual_sum(n, total):
        send_partial(n).wait_recv()
        r = res_s[:, lanes(n, 512)].astype(F32) + (
            own_s[:, lanes(n, 512)].astype(F32) + pr_in[n].astype(F32)
        )
        acc_s[:, lanes(n, 512)] = r
        return total + jnp.sum(r, axis=1, keepdims=True)

    def norm_to(target, gain_ref, total):
        mean = total * (1.0 / WIDE)

        def spread(n, s):
            d = acc_s[:, lanes(n, 512)] - mean
            return s + jnp.sum(d * d, axis=1, keepdims=True)

        var = lax.fori_loop(0, 4, spread, jnp.zeros((ROWS, 1), F32), unroll=True) * (1.0 / WIDE)
        scale = lax.rsqrt(var + EPS)

        def write(n, carry):
            d = acc_s[:, lanes(n, 512)] - mean
            target[:, lanes(n, 512)] = (d * scale * gain_ref[:, lanes(n, 512)]).astype(BF16)
            return carry

        lax.fori_loop(0, 4, write, 0, unroll=True)

    norm_to(
        normed_s, mgain_ref, lax.fori_loop(0, 4, residual_sum, jnp.zeros((ROWS, 1), F32), unroll=True)
    )

    for c in range(CHUNKS):

        def fill(n, carry):
            rows = dot(pick_s[c], normed_s[:, lanes(n, 512)])
            dsp_out[c * PER : c * PER + PER, :, lanes(n, 512)] = rows.reshape(PER, CAP, 512).astype(BF16)
            return carry

        lax.fori_loop(0, 4, fill, 0)
        for i in range(max(1, c * PER), c * PER + PER):
            pltpu.make_async_remote_copy(
                dsp_out.at[i], dsp_in.at[i], d_send, d_recv.at[c],
                device_id={"sp": shifted(me, SLOTS[i], 1)}, device_id_type=MESH,
            ).start()
    for copy in far_w:
        copy.start()
    dsp_in[0] = dsp_out[0]

    for load in loads[8:]:
        load.wait()

    def shared_inner(n, carry):
        gate = dot(normed_s[...], cg_s[:, lanes(n, 256)])
        up = dot(normed_s[...], cu_s[:, lanes(n, 256)])
        inner_s[:, lanes(n, 256)] = (silu(gate) * up).astype(BF16)
        return carry

    lax.fori_loop(0, 2, shared_inner, 0)

    def shared_down(n, carry):
        down = dot(inner_s[:, 0:512], cd_s[:, lanes(n, 512)])
        acc_s[:, lanes(n, 512)] = normed_s[:, lanes(n, 512)].astype(F32) + down
        return carry

    lax.fori_loop(0, 4, shared_down, 0)

    for copy in own_w:
        copy.wait()
    for copy in far_w:
        copy.wait()

    def arrived(buffer, c, recv):
        count = PER if c else PER - 1
        pltpu.make_async_remote_copy(
            buffer.at[pl.ds(0, count)], buffer.at[pl.ds(0, count)], d_send, recv.at[c],
            device_id={"tp": other}, device_id_type=MESH,
        ).wait_recv()

    for c in range(CHUNKS):
        arrived(dsp_in, c, d_recv)
        xb_s[...] = dsp_in[c * PER : c * PER + PER].astype(F32).reshape(ROWS, WIDE).astype(BF16)

        def inner(t, carry):
            h, n = t >> 1, t & 1
            gate = dot(xb_s[...], wg_s[h, :, lanes(n, 256)])
            up = dot(xb_s[...], wu_s[h, :, lanes(n, 256)])
            inner_s[:, lanes(t, 256)] = (silu(gate) * up).astype(BF16)
            return carry

        lax.fori_loop(0, 4, inner, 0)

        def down(n, carry):
            result = dot(inner_s[:, 0:512], wd_s[0, :, lanes(n, 512)])
            result = result + dot(inner_s[:, 512:1024], wd_s[1, :, lanes(n, 512)])
            e_out[c * PER : c * PER + PER, :, lanes(n, 512)] = result.reshape(PER, CAP, 512).astype(BF16)
            return carry

        lax.fori_loop(0, 4, down, 0)
        for i in range(max(1, c * PER), c * PER + PER):
            pltpu.make_async_remote_copy(
                e_out.at[i], ret_s.at[i], r_send, r_recv.at[c],
                device_id={"sp": shifted(me, SLOTS[i], -1)}, device_id_type=MESH,
            ).start()
    ret_s[0] = e_out[0]

    for c in range(CHUNKS):
        arrived(ret_s, c, r_recv)

        def combine(n, carry):
            rows = ret_s[c * PER : c * PER + PER, :, lanes(n, 512)]
            rows = rows.astype(F32).reshape(ROWS, 512).astype(BF16)
            parts = dot(comb_s[c], rows)
            acc_s[:, lanes(n, 512)] += parts[:ROWS] + parts[ROWS:]
            return carry

        lax.fori_loop(0, 4, combine, 0)

    def total_of(n, total):
        return total + jnp.sum(acc_s[:, lanes(n, 512)], axis=1, keepdims=True)

    norm_to(out_ref, fgain_ref, lax.fori_loop(0, 4, total_of, jnp.zeros((ROWS, 1), F32), unroll=True))

    drain(st_in, N_SP - 1, st_send, st_recv).wait_send()
    drain(tot_in, N_SP - 1, tt_send, tt_recv).wait_send()
    drain(inc_s, N_SP - 1, sc_send, sc_recv).wait_send()
    drain(dsp_in, N_SP - 1, d_send, d_recv.at[0]).wait_send()
    drain(ret_s, N_SP - 1, r_send, r_recv.at[0]).wait_send()

    def partial_left(n, carry):
        send_partial(n).wait_send()
        return carry

    lax.fori_loop(0, 4, partial_left, 0)


def per_device(
    q, k, v, g, a, x, res, hgain, wo, mgain, routes, rw, wg, wu, wd, cg, cu, cd, fgain
):
    anywhere = pl.BlockSpec(memory_space=pl.ANY)
    vmem = pl.BlockSpec(memory_space=pltpu.VMEM)
    specs = [anywhere] * 7 + [vmem, anywhere, vmem, vmem, vmem] + [anywhere] * 6 + [vmem]
    dma = pltpu.SemaphoreType.DMA
    scratch = [
        pltpu.VMEM((TOK, 1024), BF16),
        pltpu.VMEM((TOK, 1024), BF16),
        pltpu.VMEM((TOK, 1024), BF16),
        pltpu.VMEM((TOK, 1024), BF16),
        pltpu.VMEM((TOK, 1024), BF16),
        pltpu.VMEM((16, TOK), F32),
        pltpu.VMEM((ROWS, WIDE), BF16),
        pltpu.VMEM((1024, WIDE), BF16),
        pltpu.VMEM((WIDE, 512), BF16),
        pltpu.VMEM((WIDE, 512), BF16),
        pltpu.VMEM((512, WIDE), BF16),
        pltpu.VMEM((2, WIDE, 512), BF16),
        pltpu.VMEM((2, WIDE, 512), BF16),
        pltpu.VMEM((2, 512, WIDE), BF16),
        pltpu.VMEM((TOK, 1024), F32),
        pltpu.VMEM((TOK, 1024), F32),
        pltpu.VMEM((TOK, WIDE), BF16),
        pltpu.VMEM((N_SP, 16, 128), BF16),
        pltpu.VMEM((N_SP, 16, 128), BF16),
        pltpu.VMEM((PAIRS, 1, 128), F32),
        pltpu.VMEM((N_SP, 1, 128), F32),
        pltpu.VMEM((N_SP, 16, 128), BF16),
        pltpu.VMEM((N_SP, 16, 128), BF16),
        pltpu.VMEM((TOK, 1024), F32),
        pltpu.VMEM((TOK, 1024), BF16),
        pltpu.VMEM((ROWS, WIDE), BF16),
        pltpu.VMEM((4, ROWS, 512), BF16),
        pltpu.VMEM((4, ROWS, 512), BF16),
        pltpu.VMEM((ROWS, WIDE), BF16),
        pltpu.VMEM((CHUNKS, ROWS, ROWS), BF16),
        pltpu.VMEM((CHUNKS, 2 * ROWS, ROWS), BF16),
        pltpu.VMEM((N_SP, CAP, WIDE), BF16),
        pltpu.VMEM((N_SP, CAP, WIDE), BF16),
        pltpu.VMEM((ROWS, WIDE), BF16),
        pltpu.VMEM((ROWS, 1024), BF16),
        pltpu.VMEM((N_SP, CAP, WIDE), BF16),
        pltpu.VMEM((N_SP, CAP, WIDE), BF16),
        pltpu.VMEM((ROWS, WIDE), F32),
        dma((11,)), dma((3,)), dma((3,)), dma((3,)),
        dma, dma, dma, dma, dma, dma,
        dma((4,)), dma((4,)),
        dma, dma((CHUNKS,)), dma, dma((CHUNKS,)),
    ]
    return pl.pallas_call(
        layer_kernel,
        name="layer",
        out_shape=jax.ShapeDtypeStruct((ROWS, WIDE), BF16),
        in_specs=specs,
        out_specs=vmem,
        scratch_shapes=scratch,
        compiler_params=pltpu.CompilerParams(
            collective_id=0, has_side_effects=True, vmem_limit_bytes=60 * 1024 * 1024
        ),
    )(
        q, k, v, g, a, x.T, res, hgain.reshape(1, -1), wo, mgain.reshape(1, -1), routes.T, rw.T,
        wg, wu, wd, cg, cu, cd, fgain.reshape(1, -1),
    )


def solution(mesh):
    return jax.shard_map(
        per_device,
        mesh=mesh,
        in_specs=(
            P("sp", "tp"),
            P("sp", "tp"),
            P("sp", "tp"),
            P("sp", "tp"),
            P("sp", "tp"),
            P("sp", "tp"),
            P(SP_TP, None),
            P(),
            P("tp", None),
            P(),
            P(SP_TP, None),
            P(SP_TP, None),
            P("sp", None, "tp"),
            P("sp", None, "tp"),
            P("sp", "tp", None),
            P(),
            P(),
            P(),
            P(),
        ),
        out_specs=P(SP_TP, None),
        check_vma=False,
    )
```

```python
import jax
import jax.numpy as jnp
from jax import lax
from jax.experimental import pallas as pl
from jax.experimental.pallas import tpu as pltpu
from jax.sharding import PartitionSpec as P

F32 = jnp.float32
BF16 = jnp.bfloat16
MESH = pl.DeviceIdType.MESH
EPS = 1e-06
SP_TP = ("sp", "tp")

N_SP = 64
TOK = 256
ROWS = 128
PAIRS = 8
WIDE = 2048
CHUNKS = 4
PER = N_SP // CHUNKS
CAP = 8


def hops(s):
    return sum(min(d, 4 - d) for d in (s >> 4, (s >> 2) & 3, s & 3))


FAR_FIRST = sorted(range(1, N_SP), key=lambda s: -hops(s))
SLOTS = [53 * i % N_SP for i in range(N_SP)]


def dot(a, b):
    return jnp.dot(a, b, preferred_element_type=F32)


def dot_nt(a, b):
    return lax.dot_general(a, b, (((1,), (1,)), ((), ())), preferred_element_type=F32)


def dot_tn(a, b):
    return lax.dot_general(a, b, (((0,), (0,)), ((), ())), preferred_element_type=F32)


def split2(x):
    hi = x.astype(BF16)
    return hi, (x - hi.astype(F32)).astype(BF16)


def shifted(me, s, sign):
    z = ((me >> 4) + sign * (s >> 4)) & 3
    y = (((me >> 2) & 3) + sign * ((s >> 2) & 3)) & 3
    x = ((me & 3) + sign * (s & 3)) & 3
    return z * 16 + y * 4 + x


def silu(x):
    return x / (1.0 + jnp.exp(-x))


def log_sigmoid(x):
    return jnp.minimum(x, 0.0) - jnp.log(1.0 + jnp.exp(-jnp.abs(x)))


def lanes(p, width=128):
    return pl.ds(pl.multiple_of(p * width, width), width)


def iota(shape, axis):
    return lax.broadcasted_iota(jnp.int32, shape, axis)


def layer_kernel(
    q_hbm, k_hbm, v_hbm, g_hbm, a_hbm, x_hbm, res_hbm, hgain_ref, wo_hbm, mgain_ref,
    routes_ref, rw_ref, wg_hbm, wu_hbm, wd_hbm, cg_hbm, cu_hbm, cd_hbm, fgain_ref,
    out_ref,
    q_s, k_s, v_s, g_s, a_s, x_s, res_s, wo_s, cg_s, cu_s, cd_s, wg_s, wu_s, wd_s,
    from_s, local_s, qcat_s, st_out, st_in, tot_out, tot_in, sc_out, inc_s,
    gate_s, gated_s, own_s, pr_out, pr_in, normed_s, pick_s, comb_s,
    dsp_out, dsp_in, xb_s, inner_s, e_out, ret_s, acc_s,
    ld_sem, w_own_sem, w_send, w_recv, st_send, st_recv, tt_send, tt_recv, sc_send, sc_recv,
    pr_send, pr_recv, d_send, d_recv, r_send, r_recv,
):
    me = lax.axis_index("sp")
    core = lax.axis_index("tp")
    other = 1 - core

    sources = (a_hbm, x_hbm, k_hbm, v_hbm, q_hbm, g_hbm, wo_hbm, res_hbm, cg_hbm, cu_hbm, cd_hbm)
    targets = (a_s, x_s, k_s, v_s, q_s, g_s, wo_s, res_s, cg_s, cu_s, cd_s)
    loads = [
        pltpu.make_async_copy(s, t, ld_sem.at[i]) for i, (s, t) in enumerate(zip(sources, targets))
    ]
    for load in loads[:6]:
        load.start()

    barrier = pltpu.get_barrier_semaphore()

    for s in FAR_FIRST:
        pl.semaphore_signal(
            barrier, inc=1, device_id={"sp": shifted(me, s, 1)}, device_id_type=MESH
        )
    pl.semaphore_signal(barrier, inc=1, device_id={"tp": other}, device_id_type=MESH)

    low = iota((TOK, TOK), 0) >= iota((TOK, TOK), 1)
    low_bf = jnp.where(low, 1.0, 0.0).astype(BF16)
    half64 = iota((64, 128), 1) < 64
    for load in loads[:4]:
        load.wait()
    w_pairs = ((wg_hbm, wg_s), (wu_hbm, wu_s), (wd_hbm, wd_s))
    own_w = [
        pltpu.make_async_copy(s.at[0], t.at[0], w_own_sem.at[i]) for i, (s, t) in enumerate(w_pairs)
    ]
    far_w = [
        pltpu.make_async_remote_copy(
            s.at[0], t.at[1], w_send.at[i], w_recv.at[i],
            device_id={"tp": other}, device_id_type=MESH,
        )
        for i, (s, t) in enumerate(w_pairs)
    ]
    for load in loads[6:] + own_w:
        load.start()

    added_hi = x_s[...].astype(BF16)
    rest = x_s[...] - added_hi.astype(F32)
    added = jnp.concatenate([added_hi.astype(F32)] + [r.astype(F32) for r in split2(rest)], axis=0)
    added = added.T.astype(BF16)

    def own_state(p, carry):
        spread = jnp.where((iota((48, 128), 0) & 15) == 2 * p + (iota((48, 128), 1) >> 6), 1.0, 0.0)
        decay = log_sigmoid(a_s[:, lanes(p)].astype(F32)) * (1.0 / 16.0)
        decay = decay + dot(added, spread.astype(BF16))
        summed = dot(low_bf, jnp.concatenate(split2(decay), axis=1))
        total = summed[:, :128] + summed[:, 128:]
        from_s[:, lanes(p)] = total
        last = total[TOK - 1 :, :]
        tot_out[p] = jnp.exp(last)
        key = k_s[:, lanes(p)].astype(F32)
        up = (key * jnp.exp(total)).astype(BF16)
        end = (key * jnp.exp(last - total)).astype(BF16)
        state = dot_tn(v_s[:, lanes(p)], jnp.concatenate([end, up], axis=1))
        left = jnp.where(half64, state[:64, :128], state[64:, :128]).astype(BF16)
        right = jnp.where(half64, state[:64, 128:], state[64:, 128:]).astype(BF16)
        for part in range(4):
            st_out[4 * p + part] = left[16 * part : 16 * part + 16]
            st_out[32 + 4 * p + part] = right[16 * part : 16 * part + 16]
        return carry

    lax.fori_loop(0, PAIRS, own_state, 0, unroll=8)

    pl.semaphore_wait(barrier, N_SP)

    for s in FAR_FIRST:
        to = shifted(me, s, 1)
        pltpu.make_async_remote_copy(
            st_out.at[to], st_in.at[me], st_send, st_recv,
            device_id={"sp": to}, device_id_type=MESH,
        ).start()
        pltpu.make_async_remote_copy(
            tot_out.at[(to & 31) >> 2], tot_in.at[me], tt_send, tt_recv,
            device_id={"sp": to}, device_id_type=MESH,
        ).start()
    st_in[me] = st_out[me]
    tot_in[me] = tot_out[(me & 31) >> 2]

    loads[4].wait()
    even = iota((ROWS, 128), 1) < 64
    ahead_mask = iota((ROWS, 256), 0) >= (iota((ROWS, 256), 1) & (ROWS - 1))
    zero = jnp.zeros((ROWS, 128), BF16)

    def both(x):
        return jnp.concatenate([jnp.where(even, x, zero), jnp.where(even, zero, x)], axis=0)

    def local_pair(p, carry):
        total = from_s[:, lanes(p)]
        query = q_s[:, lanes(p)].astype(F32) * 0.125
        key = k_s[:, lanes(p)].astype(F32)
        value = v_s[:, lanes(p)]
        last = total[TOK - 1 :, :]
        qcat_s[:, pl.ds(pl.multiple_of(p * 256, 256), 128)] = (query * jnp.exp(total)).astype(BF16)
        qcat_s[:, pl.ds(pl.multiple_of(p * 256 + 128, 128), 128)] = (
            query * jnp.exp(last - total)
        ).astype(BF16)
        mid_total = total[ROWS - 1 : ROWS, :]
        across = jnp.exp(-jnp.abs(total - mid_total))
        query_across = (query * across).astype(BF16)
        key_across = (key * across).astype(BF16)
        for b in range(2):
            rows = slice(ROWS * b, ROWS * b + ROWS)
            far = slice(ROWS * (1 - b), ROWS * (1 - b) + ROWS)
            center = total[rows] - total[ROWS * b + 63 : ROWS * b + 64, :]
            grow = jnp.exp(center)
            fade = jnp.exp(-center)
            ahead = dot_nt((query[rows] * grow).astype(BF16), both((key[rows] * fade).astype(BF16)))
            behind = dot_nt(
                (query[rows] * fade).astype(BF16), both((key[rows] * grow).astype(BF16))
            )
            scores = jnp.where(ahead_mask, ahead, behind).astype(BF16)
            result = dot(scores, both(value[rows]))
            state = dot_tn(value[far], key_across[far])
            state = jnp.where((iota((128, 128), 0) < 64) == even, state, 0.0).astype(BF16)
            result = result + dot_nt(query_across[rows], state)
            local_s[rows, lanes(p)] = result
        return carry

    lax.fori_loop(0, PAIRS // 2, local_pair, 0)

    strict = jnp.where(iota((ROWS, ROWS), 0) < iota((ROWS, ROWS), 1), 1.0, 0.0).astype(BF16)
    slot = iota((ROWS, ROWS), 0)

    for c in range(CHUNKS):
        expert = jnp.concatenate(
            [
                jnp.full((CAP, ROWS), shifted(me, s, 1), jnp.int32)
                for s in SLOTS[PER * c : PER * c + PER]
            ],
            axis=0,
        )
        first = routes_ref[0:1, :] == expert
        second = routes_ref[1:2, :] == expert
        named = jnp.where(first | second, 1.0, 0.0)
        rank = dot(named.astype(BF16), strict)
        chosen = (named > 0.5) & (rank == (slot & (CAP - 1)).astype(F32))
        pick_s[c] = jnp.where(chosen, 1.0, 0.0).astype(BF16)
        weight = jnp.where(chosen, jnp.where(first, rw_ref[0:1, :], rw_ref[1:2, :]), 0.0).T
        weight_hi = weight.astype(BF16)
        comb_s[c, :ROWS] = weight_hi
        comb_s[c, ROWS:] = (weight - weight_hi.astype(F32)).astype(BF16)

    def drain(buffer, count, send, recv):
        done = pltpu.make_async_remote_copy(
            buffer.at[pl.ds(0, count)], buffer.at[pl.ds(0, count)], send, recv,
            device_id={"tp": other}, device_id_type=MESH,
        )
        return done

    drain(st_in, N_SP - 1, st_send, st_recv).wait_recv()
    drain(tot_in, N_SP - 1, tt_send, tt_recv).wait_recv()
    backward = me >= 32

    def scan_step(i, state):
        at = jnp.where(backward, N_SP - 1 - i, i)
        sc_out[at] = state.astype(BF16)
        return state * tot_in[at] + st_in[at].astype(F32)

    lax.fori_loop(0, N_SP, scan_step, jnp.zeros((16, 128), F32), unroll=16)

    for s in FAR_FIRST:
        to = shifted(me, s, 1)
        pltpu.make_async_remote_copy(
            sc_out.at[to], inc_s.at[me], sc_send, sc_recv,
            device_id={"sp": to}, device_id_type=MESH,
        ).start()
    inc_s[me] = sc_out[me]
    lax.fori_loop(PAIRS // 2, PAIRS, local_pair, 0)
    loads[5].wait()
    gain = jnp.concatenate([hgain_ref[...], hgain_ref[...]], axis=1)

    def gates(p, carry):
        gate_s[:, lanes(p)] = silu(g_s[:, lanes(p)].astype(F32)) * gain
        return carry

    lax.fori_loop(0, PAIRS, gates, 0)
    loads[6].wait()
    loads[7].wait()
    drain(inc_s, N_SP - 1, sc_send, sc_recv).wait_recv()

    block_mean = jnp.where(
        ((iota((TOK, 128), 0) >> 6) & 1) == (iota((TOK, 128), 1) >> 6), 1.0 / 64.0, 0.0
    ).astype(BF16)
    hzero = jnp.zeros((64, 128), BF16)

    def mix_pair(p, carry):
        left = jnp.concatenate([inc_s[4 * p + part] for part in range(4)], axis=0)
        right = jnp.concatenate([inc_s[32 + 4 * p + part] for part in range(4)], axis=0)
        state = jnp.concatenate(
            [
                jnp.concatenate([jnp.where(half64, left, hzero), jnp.where(half64, right, hzero)], axis=1),
                jnp.concatenate([jnp.where(half64, hzero, left), jnp.where(half64, hzero, right)], axis=1),
            ],
            axis=0,
        )
        mixed = local_s[:, lanes(p)] + dot_nt(qcat_s[:, lanes(p, 256)], state)
        mean = dot(jnp.concatenate(split2(mixed * mixed), axis=1), block_mean)
        gated_s[:, lanes(p)] = (mixed * lax.rsqrt(mean + EPS) * gate_s[:, lanes(p)]).astype(BF16)
        return carry

    lax.fori_loop(0, PAIRS, mix_pair, 0, unroll=8)

    def send_partial(n):
        return pltpu.make_async_remote_copy(
            pr_out.at[n], pr_in.at[n], pr_send.at[n], pr_recv.at[n],
            device_id={"tp": other}, device_id_type=MESH,
        )

    def project(n, carry):
        part = dot(gated_s[...], wo_s[:, lanes(n, 512)]).astype(BF16)
        mine, theirs = part[:ROWS], part[ROWS:]
        own_s[:, lanes(n, 512)] = jnp.where(core == 0, mine, theirs)
        pr_out[n] = jnp.where(core == 0, theirs, mine)
        send_partial(n).start()
        return carry

    lax.fori_loop(0, 4, project, 0, unroll=True)

    def residual_sum(n, total):
        send_partial(n).wait_recv()
        r = res_s[:, lanes(n, 512)].astype(F32) + (
            own_s[:, lanes(n, 512)].astype(F32) + pr_in[n].astype(F32)
        )
        acc_s[:, lanes(n, 512)] = r
        return total + jnp.sum(r, axis=1, keepdims=True)

    def norm_to(target, gain_ref, total):
        mean = total * (1.0 / WIDE)

        def spread(n, s):
            d = acc_s[:, lanes(n, 512)] - mean
            return s + jnp.sum(d * d, axis=1, keepdims=True)

        var = lax.fori_loop(0, 4, spread, jnp.zeros((ROWS, 1), F32), unroll=True) * (1.0 / WIDE)
        scale = lax.rsqrt(var + EPS)

        def write(n, carry):
            d = acc_s[:, lanes(n, 512)] - mean
            target[:, lanes(n, 512)] = (d * scale * gain_ref[:, lanes(n, 512)]).astype(BF16)
            return carry

        lax.fori_loop(0, 4, write, 0, unroll=True)

    norm_to(
        normed_s, mgain_ref, lax.fori_loop(0, 4, residual_sum, jnp.zeros((ROWS, 1), F32), unroll=True)
    )

    for c in range(CHUNKS):

        def fill(n, carry):
            rows = dot(pick_s[c], normed_s[:, lanes(n, 512)])
            dsp_out[c * PER : c * PER + PER, :, lanes(n, 512)] = rows.reshape(PER, CAP, 512).astype(BF16)
            return carry

        lax.fori_loop(0, 4, fill, 0, unroll=True)
        for i in range(max(1, c * PER), c * PER + PER):
            pltpu.make_async_remote_copy(
                dsp_out.at[i], dsp_in.at[i], d_send, d_recv.at[c],
                device_id={"sp": shifted(me, SLOTS[i], 1)}, device_id_type=MESH,
            ).start()
    for copy in far_w:
        copy.start()
    dsp_in[0] = dsp_out[0]

    for load in loads[8:]:
        load.wait()

    def shared_inner(n, carry):
        gate = dot(normed_s[...], cg_s[:, lanes(n, 256)])
        up = dot(normed_s[...], cu_s[:, lanes(n, 256)])
        inner_s[:, lanes(n, 256)] = (silu(gate) * up).astype(BF16)
        return carry

    lax.fori_loop(0, 2, shared_inner, 0)

    def shared_down(n, carry):
        down = dot(inner_s[:, 0:512], cd_s[:, lanes(n, 512)])
        acc_s[:, lanes(n, 512)] = normed_s[:, lanes(n, 512)].astype(F32) + down
        return carry

    lax.fori_loop(0, 4, shared_down, 0)

    for copy in own_w:
        copy.wait()
    for copy in far_w:
        copy.wait()

    def arrived(buffer, c, recv):
        count = PER if c else PER - 1
        pltpu.make_async_remote_copy(
            buffer.at[pl.ds(0, count)], buffer.at[pl.ds(0, count)], d_send, recv.at[c],
            device_id={"tp": other}, device_id_type=MESH,
        ).wait_recv()

    for c in range(CHUNKS):
        arrived(dsp_in, c, d_recv)
        xb_s[...] = dsp_in[c * PER : c * PER + PER].astype(F32).reshape(ROWS, WIDE).astype(BF16)

        def inner(t, carry):
            h, n = t >> 1, t & 1
            gate = dot(xb_s[...], wg_s[h, :, lanes(n, 256)])
            up = dot(xb_s[...], wu_s[h, :, lanes(n, 256)])
            inner_s[:, lanes(t, 256)] = (silu(gate) * up).astype(BF16)
            return carry

        lax.fori_loop(0, 4, inner, 0, unroll=2)

        def down(n, carry):
            result = dot(inner_s[:, 0:512], wd_s[0, :, lanes(n, 512)])
            result = result + dot(inner_s[:, 512:1024], wd_s[1, :, lanes(n, 512)])
            e_out[c * PER : c * PER + PER, :, lanes(n, 512)] = result.reshape(PER, CAP, 512).astype(BF16)
            return carry

        lax.fori_loop(0, 4, down, 0, unroll=2)
        for i in range(max(1, c * PER), c * PER + PER):
            pltpu.make_async_remote_copy(
                e_out.at[i], ret_s.at[i], r_send, r_recv.at[c],
                device_id={"sp": shifted(me, SLOTS[i], -1)}, device_id_type=MESH,
            ).start()
    ret_s[0] = e_out[0]

    for c in range(CHUNKS):
        arrived(ret_s, c, r_recv)

        def combine(n, carry):
            rows = ret_s[c * PER : c * PER + PER, :, lanes(n, 512)]
            rows = rows.astype(F32).reshape(ROWS, 512).astype(BF16)
            parts = dot(comb_s[c], rows)
            acc_s[:, lanes(n, 512)] += parts[:ROWS] + parts[ROWS:]
            return carry

        lax.fori_loop(0, 4, combine, 0, unroll=True)

    def total_of(n, total):
        return total + jnp.sum(acc_s[:, lanes(n, 512)], axis=1, keepdims=True)

    norm_to(out_ref, fgain_ref, lax.fori_loop(0, 4, total_of, jnp.zeros((ROWS, 1), F32), unroll=True))

    drain(st_in, N_SP - 1, st_send, st_recv).wait_send()
    drain(tot_in, N_SP - 1, tt_send, tt_recv).wait_send()
    drain(inc_s, N_SP - 1, sc_send, sc_recv).wait_send()
    drain(dsp_in, N_SP - 1, d_send, d_recv.at[0]).wait_send()
    drain(ret_s, N_SP - 1, r_send, r_recv.at[0]).wait_send()

    def partial_left(n, carry):
        send_partial(n).wait_send()
        return carry

    lax.fori_loop(0, 4, partial_left, 0)


def per_device(
    q, k, v, g, a, x, res, hgain, wo, mgain, routes, rw, wg, wu, wd, cg, cu, cd, fgain
):
    anywhere = pl.BlockSpec(memory_space=pl.ANY)
    vmem = pl.BlockSpec(memory_space=pltpu.VMEM)
    specs = [anywhere] * 7 + [vmem, anywhere, vmem, vmem, vmem] + [anywhere] * 6 + [vmem]
    dma = pltpu.SemaphoreType.DMA
    scratch = [
        pltpu.VMEM((TOK, 1024), BF16),
        pltpu.VMEM((TOK, 1024), BF16),
        pltpu.VMEM((TOK, 1024), BF16),
        pltpu.VMEM((TOK, 1024), BF16),
        pltpu.VMEM((TOK, 1024), BF16),
        pltpu.VMEM((16, TOK), F32),
        pltpu.VMEM((ROWS, WIDE), BF16),
        pltpu.VMEM((1024, WIDE), BF16),
        pltpu.VMEM((WIDE, 512), BF16),
        pltpu.VMEM((WIDE, 512), BF16),
        pltpu.VMEM((512, WIDE), BF16),
        pltpu.VMEM((2, WIDE, 512), BF16),
        pltpu.VMEM((2, WIDE, 512), BF16),
        pltpu.VMEM((2, 512, WIDE), BF16),
        pltpu.VMEM((TOK, 1024), F32),
        pltpu.VMEM((TOK, 1024), F32),
        pltpu.VMEM((TOK, WIDE), BF16),
        pltpu.VMEM((N_SP, 16, 128), BF16),
        pltpu.VMEM((N_SP, 16, 128), BF16),
        pltpu.VMEM((PAIRS, 1, 128), F32),
        pltpu.VMEM((N_SP, 1, 128), F32),
        pltpu.VMEM((N_SP, 16, 128), BF16),
        pltpu.VMEM((N_SP, 16, 128), BF16),
        pltpu.VMEM((TOK, 1024), F32),
        pltpu.VMEM((TOK, 1024), BF16),
        pltpu.VMEM((ROWS, WIDE), BF16),
        pltpu.VMEM((4, ROWS, 512), BF16),
        pltpu.VMEM((4, ROWS, 512), BF16),
        pltpu.VMEM((ROWS, WIDE), BF16),
        pltpu.VMEM((CHUNKS, ROWS, ROWS), BF16),
        pltpu.VMEM((CHUNKS, 2 * ROWS, ROWS), BF16),
        pltpu.VMEM((N_SP, CAP, WIDE), BF16),
        pltpu.VMEM((N_SP, CAP, WIDE), BF16),
        pltpu.VMEM((ROWS, WIDE), BF16),
        pltpu.VMEM((ROWS, 1024), BF16),
        pltpu.VMEM((N_SP, CAP, WIDE), BF16),
        pltpu.VMEM((N_SP, CAP, WIDE), BF16),
        pltpu.VMEM((ROWS, WIDE), F32),
        dma((11,)), dma((3,)), dma((3,)), dma((3,)),
        dma, dma, dma, dma, dma, dma,
        dma((4,)), dma((4,)),
        dma, dma((CHUNKS,)), dma, dma((CHUNKS,)),
    ]
    return pl.pallas_call(
        layer_kernel,
        name="layer",
        out_shape=jax.ShapeDtypeStruct((ROWS, WIDE), BF16),
        in_specs=specs,
        out_specs=vmem,
        scratch_shapes=scratch,
        compiler_params=pltpu.CompilerParams(
            collective_id=0, has_side_effects=True, vmem_limit_bytes=60 * 1024 * 1024
        ),
    )(
        q, k, v, g, a, x.T, res, hgain.reshape(1, -1), wo, mgain.reshape(1, -1), routes.T, rw.T,
        wg, wu, wd, cg, cu, cd, fgain.reshape(1, -1),
    )


def solution(mesh):
    return jax.shard_map(
        per_device,
        mesh=mesh,
        in_specs=(
            P("sp", "tp"),
            P("sp", "tp"),
            P("sp", "tp"),
            P("sp", "tp"),
            P("sp", "tp"),
            P("sp", "tp"),
            P(SP_TP, None),
            P(),
            P("tp", None),
            P(),
            P(SP_TP, None),
            P(SP_TP, None),
            P("sp", None, "tp"),
            P("sp", None, "tp"),
            P("sp", "tp", None),
            P(),
            P(),
            P(),
            P(),
        ),
        out_specs=P(SP_TP, None),
        check_vma=False,
    )
```

```python
import jax
import jax.numpy as jnp
from jax import lax
from jax.experimental import pallas as pl
from jax.experimental.pallas import tpu as pltpu
from jax.sharding import PartitionSpec as P

F32 = jnp.float32
BF16 = jnp.bfloat16
MESH = pl.DeviceIdType.MESH
EPS = 1e-06
SP_TP = ("sp", "tp")

N_SP = 64
TOK = 256
ROWS = 128
PAIRS = 8
WIDE = 2048
CHUNKS = 4
PER = N_SP // CHUNKS
CAP = 8


def hops(s):
    return sum(min(d, 4 - d) for d in (s >> 4, (s >> 2) & 3, s & 3))


FAR_FIRST = sorted(range(1, N_SP), key=lambda s: -hops(s))
SLOTS = [53 * i % N_SP for i in range(N_SP)]


def dot(a, b):
    return jnp.dot(a, b, preferred_element_type=F32)


def dot_nt(a, b):
    return lax.dot_general(a, b, (((1,), (1,)), ((), ())), preferred_element_type=F32)


def dot_tn(a, b):
    return lax.dot_general(a, b, (((0,), (0,)), ((), ())), preferred_element_type=F32)


def split2(x):
    hi = x.astype(BF16)
    return hi, (x - hi.astype(F32)).astype(BF16)


def shifted(me, s, sign):
    z = ((me >> 4) + sign * (s >> 4)) & 3
    y = (((me >> 2) & 3) + sign * ((s >> 2) & 3)) & 3
    x = ((me & 3) + sign * (s & 3)) & 3
    return z * 16 + y * 4 + x


def silu(x):
    return x / (1.0 + jnp.exp(-x))


def log_sigmoid(x):
    return jnp.minimum(x, 0.0) - jnp.log(1.0 + jnp.exp(-jnp.abs(x)))


def lanes(p, width=128):
    return pl.ds(pl.multiple_of(p * width, width), width)


def iota(shape, axis):
    return lax.broadcasted_iota(jnp.int32, shape, axis)


def layer_kernel(
    q_hbm, k_hbm, v_hbm, g_hbm, a_hbm, x_hbm, res_hbm, hgain_ref, wo_hbm, mgain_ref,
    routes_ref, rw_ref, wg_hbm, wu_hbm, wd_hbm, cg_hbm, cu_hbm, cd_hbm, fgain_ref,
    out_ref,
    q_s, k_s, v_s, g_s, a_s, x_s, res_s, wo_s, cg_s, cu_s, cd_s, wg_s, wu_s, wd_s,
    from_s, local_s, qcat_s, st_out, st_in, tot_out, tot_in, sc_out, inc_s,
    gate_s, gated_s, own_s, pr_out, pr_in, normed_s, pick_s, comb_s,
    dsp_out, dsp_in, xb_s, inner_s, e_out, ret_s, acc_s,
    ld_sem, w_own_sem, w_send, w_recv, st_send, st_recv, tt_send, tt_recv, sc_send, sc_recv,
    pr_send, pr_recv, d_send, d_recv, r_send, r_recv,
):
    me = lax.axis_index("sp")
    core = lax.axis_index("tp")
    other = 1 - core

    sources = (a_hbm, x_hbm, k_hbm, v_hbm, q_hbm, g_hbm, wo_hbm, res_hbm, cg_hbm, cu_hbm, cd_hbm)
    targets = (a_s, x_s, k_s, v_s, q_s, g_s, wo_s, res_s, cg_s, cu_s, cd_s)
    loads = [
        pltpu.make_async_copy(s, t, ld_sem.at[i]) for i, (s, t) in enumerate(zip(sources, targets))
    ]
    for load in loads[:6]:
        load.start()

    barrier = pltpu.get_barrier_semaphore()

    for s in FAR_FIRST:
        pl.semaphore_signal(
            barrier, inc=1, device_id={"sp": shifted(me, s, 1)}, device_id_type=MESH
        )
    pl.semaphore_signal(barrier, inc=1, device_id={"tp": other}, device_id_type=MESH)

    low = iota((TOK, TOK), 0) >= iota((TOK, TOK), 1)
    low_bf = jnp.where(low, 1.0, 0.0).astype(BF16)
    half64 = iota((64, 128), 1) < 64
    for load in loads[:4]:
        load.wait()
    w_pairs = ((wg_hbm, wg_s), (wu_hbm, wu_s), (wd_hbm, wd_s))
    own_w = [
        pltpu.make_async_copy(s.at[0], t.at[0], w_own_sem.at[i]) for i, (s, t) in enumerate(w_pairs)
    ]
    far_w = [
        pltpu.make_async_remote_copy(
            s.at[0], t.at[1], w_send.at[i], w_recv.at[i],
            device_id={"tp": other}, device_id_type=MESH,
        )
        for i, (s, t) in enumerate(w_pairs)
    ]
    for load in loads[6:] + own_w:
        load.start()

    added_hi = x_s[...].astype(BF16)
    rest = x_s[...] - added_hi.astype(F32)
    added = jnp.concatenate([added_hi.astype(F32)] + [r.astype(F32) for r in split2(rest)], axis=0)
    added = added.T.astype(BF16)

    def own_state(p, carry):
        spread = jnp.where((iota((48, 128), 0) & 15) == 2 * p + (iota((48, 128), 1) >> 6), 1.0, 0.0)
        decay = log_sigmoid(a_s[:, lanes(p)].astype(F32)) * (1.0 / 16.0)
        decay = decay + dot(added, spread.astype(BF16))
        summed = dot(low_bf, jnp.concatenate(split2(decay), axis=1))
        total = summed[:, :128] + summed[:, 128:]
        from_s[:, lanes(p)] = total
        last = total[TOK - 1 :, :]
        tot_out[p] = jnp.exp(last)
        key = k_s[:, lanes(p)].astype(F32)
        up = (key * jnp.exp(total)).astype(BF16)
        end = (key * jnp.exp(last - total)).astype(BF16)
        state = dot_tn(v_s[:, lanes(p)], jnp.concatenate([end, up], axis=1))
        left = jnp.where(half64, state[:64, :128], state[64:, :128]).astype(BF16)
        right = jnp.where(half64, state[:64, 128:], state[64:, 128:]).astype(BF16)
        for part in range(4):
            st_out[4 * p + part] = left[16 * part : 16 * part + 16]
            st_out[32 + 4 * p + part] = right[16 * part : 16 * part + 16]
        return carry

    lax.fori_loop(0, PAIRS, own_state, 0, unroll=8)

    pl.semaphore_wait(barrier, N_SP)

    for s in FAR_FIRST:
        to = shifted(me, s, 1)
        pltpu.make_async_remote_copy(
            st_out.at[to], st_in.at[me], st_send, st_recv,
            device_id={"sp": to}, device_id_type=MESH,
        ).start()
        pltpu.make_async_remote_copy(
            tot_out.at[(to & 31) >> 2], tot_in.at[me], tt_send, tt_recv,
            device_id={"sp": to}, device_id_type=MESH,
        ).start()
    st_in[me] = st_out[me]
    tot_in[me] = tot_out[(me & 31) >> 2]

    loads[4].wait()
    even = iota((ROWS, 128), 1) < 64
    ahead_mask = iota((ROWS, 256), 0) >= (iota((ROWS, 256), 1) & (ROWS - 1))
    zero = jnp.zeros((ROWS, 128), BF16)

    def both(x):
        return jnp.concatenate([jnp.where(even, x, zero), jnp.where(even, zero, x)], axis=0)

    def local_pair(p, carry):
        total = from_s[:, lanes(p)]
        query = q_s[:, lanes(p)].astype(F32) * 0.125
        key = k_s[:, lanes(p)].astype(F32)
        value = v_s[:, lanes(p)]
        last = total[TOK - 1 :, :]
        qcat_s[:, pl.ds(pl.multiple_of(p * 256, 256), 128)] = (query * jnp.exp(total)).astype(BF16)
        qcat_s[:, pl.ds(pl.multiple_of(p * 256 + 128, 128), 128)] = (
            query * jnp.exp(last - total)
        ).astype(BF16)
        mid_total = total[ROWS - 1 : ROWS, :]
        across = jnp.exp(-jnp.abs(total - mid_total))
        query_across = (query * across).astype(BF16)
        key_across = (key * across).astype(BF16)
        for b in range(2):
            rows = slice(ROWS * b, ROWS * b + ROWS)
            far = slice(ROWS * (1 - b), ROWS * (1 - b) + ROWS)
            center = total[rows] - total[ROWS * b + 63 : ROWS * b + 64, :]
            grow = jnp.exp(center)
            fade = jnp.exp(-center)
            ahead = dot_nt((query[rows] * grow).astype(BF16), both((key[rows] * fade).astype(BF16)))
            behind = dot_nt(
                (query[rows] * fade).astype(BF16), both((key[rows] * grow).astype(BF16))
            )
            scores = jnp.where(ahead_mask, ahead, behind).astype(BF16)
            result = dot(scores, both(value[rows]))
            state = dot_tn(value[far], key_across[far])
            state = jnp.where((iota((128, 128), 0) < 64) == even, state, 0.0).astype(BF16)
            result = result + dot_nt(query_across[rows], state)
            local_s[rows, lanes(p)] = result
        return carry

    lax.fori_loop(0, PAIRS // 2, local_pair, 0, unroll=2)

    strict = jnp.where(iota((ROWS, ROWS), 0) < iota((ROWS, ROWS), 1), 1.0, 0.0).astype(BF16)
    slot = iota((ROWS, ROWS), 0)

    for c in range(CHUNKS):
        expert = jnp.concatenate(
            [
                jnp.full((CAP, ROWS), shifted(me, s, 1), jnp.int32)
                for s in SLOTS[PER * c : PER * c + PER]
            ],
            axis=0,
        )
        first = routes_ref[0:1, :] == expert
        second = routes_ref[1:2, :] == expert
        named = jnp.where(first | second, 1.0, 0.0)
        rank = dot(named.astype(BF16), strict)
        chosen = (named > 0.5) & (rank == (slot & (CAP - 1)).astype(F32))
        pick_s[c] = jnp.where(chosen, 1.0, 0.0).astype(BF16)
        weight = jnp.where(chosen, jnp.where(first, rw_ref[0:1, :], rw_ref[1:2, :]), 0.0).T
        weight_hi = weight.astype(BF16)
        comb_s[c, :ROWS] = weight_hi
        comb_s[c, ROWS:] = (weight - weight_hi.astype(F32)).astype(BF16)

    def drain(buffer, count, send, recv):
        done = pltpu.make_async_remote_copy(
            buffer.at[pl.ds(0, count)], buffer.at[pl.ds(0, count)], send, recv,
            device_id={"tp": other}, device_id_type=MESH,
        )
        return done

    drain(st_in, N_SP - 1, st_send, st_recv).wait_recv()
    drain(tot_in, N_SP - 1, tt_send, tt_recv).wait_recv()
    backward = me >= 32

    def scan_step(i, state):
        at = jnp.where(backward, N_SP - 1 - i, i)
        sc_out[at] = state.astype(BF16)
        return state * tot_in[at] + st_in[at].astype(F32)

    lax.fori_loop(0, N_SP, scan_step, jnp.zeros((16, 128), F32), unroll=64)

    for s in FAR_FIRST:
        to = shifted(me, s, 1)
        pltpu.make_async_remote_copy(
            sc_out.at[to], inc_s.at[me], sc_send, sc_recv,
            device_id={"sp": to}, device_id_type=MESH,
        ).start()
    inc_s[me] = sc_out[me]
    lax.fori_loop(PAIRS // 2, PAIRS, local_pair, 0, unroll=2)
    loads[5].wait()
    gain = jnp.concatenate([hgain_ref[...], hgain_ref[...]], axis=1)

    def gates(p, carry):
        gate_s[:, lanes(p)] = silu(g_s[:, lanes(p)].astype(F32)) * gain
        return carry

    lax.fori_loop(0, PAIRS, gates, 0)
    loads[6].wait()
    loads[7].wait()
    drain(inc_s, N_SP - 1, sc_send, sc_recv).wait_recv()

    block_mean = jnp.where(
        ((iota((TOK, 128), 0) >> 6) & 1) == (iota((TOK, 128), 1) >> 6), 1.0 / 64.0, 0.0
    ).astype(BF16)
    hzero = jnp.zeros((64, 128), BF16)

    def mix_pair(p, carry):
        left = jnp.concatenate([inc_s[4 * p + part] for part in range(4)], axis=0)
        right = jnp.concatenate([inc_s[32 + 4 * p + part] for part in range(4)], axis=0)
        state = jnp.concatenate(
            [
                jnp.concatenate([jnp.where(half64, left, hzero), jnp.where(half64, right, hzero)], axis=1),
                jnp.concatenate([jnp.where(half64, hzero, left), jnp.where(half64, hzero, right)], axis=1),
            ],
            axis=0,
        )
        mixed = local_s[:, lanes(p)] + dot_nt(qcat_s[:, lanes(p, 256)], state)
        mean = dot(jnp.concatenate(split2(mixed * mixed), axis=1), block_mean)
        gated_s[:, lanes(p)] = (mixed * lax.rsqrt(mean + EPS) * gate_s[:, lanes(p)]).astype(BF16)
        return carry

    lax.fori_loop(0, PAIRS, mix_pair, 0, unroll=8)

    def send_partial(n):
        return pltpu.make_async_remote_copy(
            pr_out.at[n], pr_in.at[n], pr_send.at[n], pr_recv.at[n],
            device_id={"tp": other}, device_id_type=MESH,
        )

    def project(n, carry):
        part = dot(gated_s[...], wo_s[:, lanes(n, 512)]).astype(BF16)
        mine, theirs = part[:ROWS], part[ROWS:]
        own_s[:, lanes(n, 512)] = jnp.where(core == 0, mine, theirs)
        pr_out[n] = jnp.where(core == 0, theirs, mine)
        send_partial(n).start()
        return carry

    lax.fori_loop(0, 4, project, 0, unroll=True)

    def residual_sum(n, total):
        send_partial(n).wait_recv()
        r = res_s[:, lanes(n, 512)].astype(F32) + (
            own_s[:, lanes(n, 512)].astype(F32) + pr_in[n].astype(F32)
        )
        acc_s[:, lanes(n, 512)] = r
        return total + jnp.sum(r, axis=1, keepdims=True)

    def norm_to(target, gain_ref, total):
        mean = total * (1.0 / WIDE)

        def spread(n, s):
            d = acc_s[:, lanes(n, 512)] - mean
            return s + jnp.sum(d * d, axis=1, keepdims=True)

        var = lax.fori_loop(0, 4, spread, jnp.zeros((ROWS, 1), F32), unroll=True) * (1.0 / WIDE)
        scale = lax.rsqrt(var + EPS)

        def write(n, carry):
            d = acc_s[:, lanes(n, 512)] - mean
            target[:, lanes(n, 512)] = (d * scale * gain_ref[:, lanes(n, 512)]).astype(BF16)
            return carry

        lax.fori_loop(0, 4, write, 0, unroll=True)

    norm_to(
        normed_s, mgain_ref, lax.fori_loop(0, 4, residual_sum, jnp.zeros((ROWS, 1), F32), unroll=True)
    )

    for c in range(CHUNKS):

        def fill(n, carry):
            rows = dot(pick_s[c], normed_s[:, lanes(n, 512)])
            dsp_out[c * PER : c * PER + PER, :, lanes(n, 512)] = rows.reshape(PER, CAP, 512).astype(BF16)
            return carry

        lax.fori_loop(0, 4, fill, 0, unroll=True)
        for i in range(max(1, c * PER), c * PER + PER):
            pltpu.make_async_remote_copy(
                dsp_out.at[i], dsp_in.at[i], d_send, d_recv.at[c],
                device_id={"sp": shifted(me, SLOTS[i], 1)}, device_id_type=MESH,
            ).start()
    for copy in far_w:
        copy.start()
    dsp_in[0] = dsp_out[0]

    for load in loads[8:]:
        load.wait()

    def shared_inner(n, carry):
        gate = dot(normed_s[...], cg_s[:, lanes(n, 256)])
        up = dot(normed_s[...], cu_s[:, lanes(n, 256)])
        inner_s[:, lanes(n, 256)] = (silu(gate) * up).astype(BF16)
        return carry

    lax.fori_loop(0, 2, shared_inner, 0)

    def shared_down(n, carry):
        down = dot(inner_s[:, 0:512], cd_s[:, lanes(n, 512)])
        acc_s[:, lanes(n, 512)] = normed_s[:, lanes(n, 512)].astype(F32) + down
        return carry

    lax.fori_loop(0, 4, shared_down, 0)

    for copy in own_w:
        copy.wait()
    for copy in far_w:
        copy.wait()

    def arrived(buffer, c, recv):
        count = PER if c else PER - 1
        pltpu.make_async_remote_copy(
            buffer.at[pl.ds(0, count)], buffer.at[pl.ds(0, count)], d_send, recv.at[c],
            device_id={"tp": other}, device_id_type=MESH,
        ).wait_recv()

    for c in range(CHUNKS):
        arrived(dsp_in, c, d_recv)
        xb_s[...] = dsp_in[c * PER : c * PER + PER].astype(F32).reshape(ROWS, WIDE).astype(BF16)

        def inner(t, carry):
            h, n = t >> 1, t & 1
            gate = dot(xb_s[...], wg_s[h, :, lanes(n, 256)])
            up = dot(xb_s[...], wu_s[h, :, lanes(n, 256)])
            inner_s[:, lanes(t, 256)] = (silu(gate) * up).astype(BF16)
            return carry

        lax.fori_loop(0, 4, inner, 0, unroll=2)

        def down(n, carry):
            result = dot(inner_s[:, 0:512], wd_s[0, :, lanes(n, 512)])
            result = result + dot(inner_s[:, 512:1024], wd_s[1, :, lanes(n, 512)])
            e_out[c * PER : c * PER + PER, :, lanes(n, 512)] = result.reshape(PER, CAP, 512).astype(BF16)
            return carry

        lax.fori_loop(0, 4, down, 0, unroll=2)
        for i in range(max(1, c * PER), c * PER + PER):
            pltpu.make_async_remote_copy(
                e_out.at[i], ret_s.at[i], r_send, r_recv.at[c],
                device_id={"sp": shifted(me, SLOTS[i], -1)}, device_id_type=MESH,
            ).start()
    ret_s[0] = e_out[0]

    for c in range(CHUNKS):
        arrived(ret_s, c, r_recv)

        def combine(n, carry):
            rows = ret_s[c * PER : c * PER + PER, :, lanes(n, 512)]
            rows = rows.astype(F32).reshape(ROWS, 512).astype(BF16)
            parts = dot(comb_s[c], rows)
            sums = acc_s[:, lanes(n, 512)] + (parts[:ROWS] + parts[ROWS:])
            acc_s[:, lanes(n, 512)] = sums
            return carry + jnp.sum(sums, axis=1, keepdims=True) if c == CHUNKS - 1 else carry

        row_sums = lax.fori_loop(0, 4, combine, jnp.zeros((ROWS, 1), F32), unroll=True)

    norm_to(out_ref, fgain_ref, row_sums)

    drain(st_in, N_SP - 1, st_send, st_recv).wait_send()
    drain(tot_in, N_SP - 1, tt_send, tt_recv).wait_send()
    drain(inc_s, N_SP - 1, sc_send, sc_recv).wait_send()
    drain(dsp_in, N_SP - 1, d_send, d_recv.at[0]).wait_send()
    drain(ret_s, N_SP - 1, r_send, r_recv.at[0]).wait_send()

    def partial_left(n, carry):
        send_partial(n).wait_send()
        return carry

    lax.fori_loop(0, 4, partial_left, 0)


def per_device(
    q, k, v, g, a, x, res, hgain, wo, mgain, routes, rw, wg, wu, wd, cg, cu, cd, fgain
):
    anywhere = pl.BlockSpec(memory_space=pl.ANY)
    vmem = pl.BlockSpec(memory_space=pltpu.VMEM)
    specs = [anywhere] * 7 + [vmem, anywhere, vmem, vmem, vmem] + [anywhere] * 6 + [vmem]
    dma = pltpu.SemaphoreType.DMA
    scratch = [
        pltpu.VMEM((TOK, 1024), BF16),
        pltpu.VMEM((TOK, 1024), BF16),
        pltpu.VMEM((TOK, 1024), BF16),
        pltpu.VMEM((TOK, 1024), BF16),
        pltpu.VMEM((TOK, 1024), BF16),
        pltpu.VMEM((16, TOK), F32),
        pltpu.VMEM((ROWS, WIDE), BF16),
        pltpu.VMEM((1024, WIDE), BF16),
        pltpu.VMEM((WIDE, 512), BF16),
        pltpu.VMEM((WIDE, 512), BF16),
        pltpu.VMEM((512, WIDE), BF16),
        pltpu.VMEM((2, WIDE, 512), BF16),
        pltpu.VMEM((2, WIDE, 512), BF16),
        pltpu.VMEM((2, 512, WIDE), BF16),
        pltpu.VMEM((TOK, 1024), F32),
        pltpu.VMEM((TOK, 1024), F32),
        pltpu.VMEM((TOK, WIDE), BF16),
        pltpu.VMEM((N_SP, 16, 128), BF16),
        pltpu.VMEM((N_SP, 16, 128), BF16),
        pltpu.VMEM((PAIRS, 1, 128), F32),
        pltpu.VMEM((N_SP, 1, 128), F32),
        pltpu.VMEM((N_SP, 16, 128), BF16),
        pltpu.VMEM((N_SP, 16, 128), BF16),
        pltpu.VMEM((TOK, 1024), F32),
        pltpu.VMEM((TOK, 1024), BF16),
        pltpu.VMEM((ROWS, WIDE), BF16),
        pltpu.VMEM((4, ROWS, 512), BF16),
        pltpu.VMEM((4, ROWS, 512), BF16),
        pltpu.VMEM((ROWS, WIDE), BF16),
        pltpu.VMEM((CHUNKS, ROWS, ROWS), BF16),
        pltpu.VMEM((CHUNKS, 2 * ROWS, ROWS), BF16),
        pltpu.VMEM((N_SP, CAP, WIDE), BF16),
        pltpu.VMEM((N_SP, CAP, WIDE), BF16),
        pltpu.VMEM((ROWS, WIDE), BF16),
        pltpu.VMEM((ROWS, 1024), BF16),
        pltpu.VMEM((N_SP, CAP, WIDE), BF16),
        pltpu.VMEM((N_SP, CAP, WIDE), BF16),
        pltpu.VMEM((ROWS, WIDE), F32),
        dma((11,)), dma((3,)), dma((3,)), dma((3,)),
        dma, dma, dma, dma, dma, dma,
        dma((4,)), dma((4,)),
        dma, dma((CHUNKS,)), dma, dma((CHUNKS,)),
    ]
    return pl.pallas_call(
        layer_kernel,
        name="layer",
        out_shape=jax.ShapeDtypeStruct((ROWS, WIDE), BF16),
        in_specs=specs,
        out_specs=vmem,
        scratch_shapes=scratch,
        compiler_params=pltpu.CompilerParams(
            collective_id=0, has_side_effects=True, vmem_limit_bytes=60 * 1024 * 1024
        ),
    )(
        q, k, v, g, a, x.T, res, hgain.reshape(1, -1), wo, mgain.reshape(1, -1), routes.T, rw.T,
        wg, wu, wd, cg, cu, cd, fgain.reshape(1, -1),
    )


def solution(mesh):
    return jax.shard_map(
        per_device,
        mesh=mesh,
        in_specs=(
            P("sp", "tp"),
            P("sp", "tp"),
            P("sp", "tp"),
            P("sp", "tp"),
            P("sp", "tp"),
            P("sp", "tp"),
            P(SP_TP, None),
            P(),
            P("tp", None),
            P(),
            P(SP_TP, None),
            P(SP_TP, None),
            P("sp", None, "tp"),
            P("sp", None, "tp"),
            P("sp", "tp", None),
            P(),
            P(),
            P(),
            P(),
        ),
        out_specs=P(SP_TP, None),
        check_vma=False,
    )
```
